32 devices in a mesh: ep: 16 (over z, y, core), tp: 2 (over x).
Axes of the slice: x: 2, y: 2, z: 4, core: 2. Of those that a mesh axis runs over, the one named last changes fastest.
Arguments:
- resid: bfloat16 [256, 2048], P('ep'), may hold values from -40 to 40
- queries: bfloat16 [256, 1024], P('ep', 'tp'), may hold values from -146 to 146
- new_keys: bfloat16 [256, 512], P('ep', 'tp'), may hold values from -6 to 6
- new_values: bfloat16 [256, 512], P('ep', 'tp'), may hold values from -18 to 18
- key_cache: bfloat16 [256, 4, 256, 128], P('ep', 'tp'), may hold values from -5 to 5
- value_cache: bfloat16 [256, 4, 256, 128], P('ep', 'tp'), may hold values from -18 to 18
- cum_gate: float32 [256, 8, 256], P('ep', 'tp'), may hold values from -256 to 0, as said below
- forget_logit: float32 [256, 8], P('ep', 'tp'), may hold values from -6 to 6
- forget_bias: float32 [8], P('tp'), may hold values from -3 to 2
- lengths: int32 [256], P('ep'), may hold values from 32 to 256
- out_weight: bfloat16 [1024, 2048], P('tp'), may hold values from -0.1875 to 0.1875
- norm_gain: float32 [2048], replicated, may hold values from 0.1 to 1.9
- mix_vector: bfloat16 [2048], replicated, may hold values from -0.125 to 0.125
- routes: int32 [256, 2], P('ep'), may hold values from 0 to 3, all different within a row; in each aligned block of 16 rows (0 to 15, 16 to 31, ...) at most 16 rows name the same one
- route_weight: float32 [256, 2], P('ep'), may hold values from 0.2 to 1
- expert_gate: bfloat16 [16, 2048, 768], P('ep', 'tp'), may hold values from -0.125 to 0.125
- expert_up: bfloat16 [16, 2048, 768], P('ep', 'tp'), may hold values from -0.125 to 0.125
- expert_down: bfloat16 [16, 768, 2048], P('ep', None, 'tp'), may hold values from -0.109375 to 0.109375
- dense_gate: bfloat16 [2048, 3072], P('tp', 'ep'), may hold values from -0.125 to 0.125
- dense_up: bfloat16 [2048, 3072], P('tp', 'ep'), may hold values from -0.125 to 0.125
- dense_down: bfloat16 [3072, 2048], P('ep', 'tp'), may hold values from -0.109375 to 0.109375
Outputs:
- layer_out: bfloat16 [256, 2048], P('ep', 'tp')
The draws below stay inside these ranges and needn't reach their ends.
Inputs may be any that keep to these rules, and one draw needn't show every extreme that they name: `routes`: each row names 2 different experts; the rows of one index of ep name no expert more than 16 times. `cum_gate`: for positions below the sequence's length, the running sum of the log forget gates of positions 0 to p; it never rises along p.
All inputs are finite; a program needn't handle non-finite values.
Results may differ from the reference program's by a relative error of at most 0.0095.
Values may be sent and summed in bfloat16 or wider, within the bound.
A program may use at most 64 MiB of HBM per device.

```python
import math
import jax
import jax.numpy as jnp
import numpy as np
from jax import lax

D = 2048
QUERY_HEADS = 8
KV_HEADS = 4
HEAD = 128
FF = 3072
FFD = 3072
TOP_K = 2
EXP_SPAN = 4
SEQ_DEV = 16
CACHE_SLOTS = 256
SEQUENCE_TOTAL = 256
EXPERTS = 4
CAP = 16
FF_SPAN = 768
N_EP = 16
N_TP = 2


def first_keys(key):
    return jnp.clip(jax.random.normal(jax.random.fold_in(key, 11), (SEQUENCE_TOTAL, KV_HEADS, HEAD), jnp.float32), -5.0, 5.0)


def draw_key_cache(key, part):
    leading = first_keys(key)
    others = jnp.clip(jax.random.normal(jax.random.fold_in(key, 12), (SEQUENCE_TOTAL, KV_HEADS, CACHE_SLOTS, HEAD), jnp.float32), -5.0, 5.0)
    full = others.at[:, :, 0, :].set(leading)
    return full.astype(jnp.bfloat16)


def draw_queries(key, part):
    base = jnp.clip(jax.random.normal(jax.random.fold_in(key, 15), (SEQUENCE_TOTAL, QUERY_HEADS, HEAD), jnp.float32), -5.0, 5.0)
    return base.reshape(SEQUENCE_TOTAL, QUERY_HEADS * HEAD).astype(jnp.bfloat16)


def draw_resid(key, part):
    block_index = jnp.arange(D) * N_TP // D
    rising = 3.0 ** (block_index.astype(jnp.float32) / max(N_TP - 1, 1))
    column = jnp.exp(jax.random.uniform(jax.random.fold_in(key, 21), (D,), jnp.float32, 0.0, math.log(3.0)))
    base = jnp.clip(jax.random.normal(jax.random.fold_in(key, 22), (SEQUENCE_TOTAL, D), jnp.float32), -4.0, 4.0)
    rowscale = jnp.exp(jax.random.uniform(jax.random.fold_in(key, 23), (SEQUENCE_TOTAL,), jnp.float32, math.log(0.3), math.log(3.0)))
    values = base * rowscale[:, None] * (column * rising)[None, :] / 3.0
    return jnp.clip(values, -40.0, 40.0).astype(jnp.bfloat16)


def draw_cum_gate(key, part):
    slow_share = 0.5
    slower_path = jax.random.uniform(jax.random.fold_in(key, 31), (SEQUENCE_TOTAL, QUERY_HEADS, 1), jnp.float32) < slow_share
    whole_loss = jnp.exp(jax.random.uniform(jax.random.fold_in(key, 32), (SEQUENCE_TOTAL, QUERY_HEADS, 1), jnp.float32, math.log(0.5), math.log(2.0)))
    fast_rate = jnp.exp(jax.random.uniform(jax.random.fold_in(key, 33), (SEQUENCE_TOTAL, QUERY_HEADS, 1), jnp.float32, math.log(0.01), math.log(1.0 / 30.0)))
    decay_rate = jnp.where(slower_path, whole_loss / CACHE_SLOTS, fast_rate)
    coarse_estimate = jax.random.uniform(jax.random.fold_in(key, 34), (SEQUENCE_TOTAL, QUERY_HEADS, CACHE_SLOTS), jnp.float32, 0.2, 1.8)
    quarter = jnp.exp(jax.random.uniform(jax.random.fold_in(key, 35), (SEQUENCE_TOTAL, QUERY_HEADS, 4), jnp.float32, math.log(0.5), math.log(2.0)))
    per_block_pass = jnp.repeat(quarter, CACHE_SLOTS // 4, axis=2)
    sudden_spike = jax.random.uniform(jax.random.fold_in(key, 36), (SEQUENCE_TOTAL, QUERY_HEADS, CACHE_SLOTS), jnp.float32) < 3.0 / CACHE_SLOTS
    dropped_amount = jnp.log(jax.random.uniform(jax.random.fold_in(key, 37), (SEQUENCE_TOTAL, QUERY_HEADS, CACHE_SLOTS), jnp.float32, 0.5, 0.8))
    decode_steps = -decay_rate * coarse_estimate * per_block_pass + jnp.where(sudden_spike & slower_path, dropped_amount, 0.0)
    return jnp.cumsum(decode_steps, axis=2).astype(jnp.float32)


def touch_ends(values, key, low, high):
    longest = values.shape.index(max(values.shape))
    spots = []
    for shift in (0, 1):
        where = [jax.random.randint(jax.random.fold_in(key, axis), (), 0, length) for axis, length in enumerate(values.shape)]
        where[longest] = (where[longest] + shift) % values.shape[longest]
        spots.append(tuple(where))
    return values.at[spots[0]].set(low).at[spots[1]].set(high)


def steps_of(key, dims, cuts, smallest, high):
    def one(dim, shards_of):
        draws = jax.random.uniform(jax.random.fold_in(jax.random.fold_in(key, 6), dim), (shards_of,), jnp.float32, smallest / len(cuts), high / len(cuts))
        return jnp.repeat(jnp.exp(draws), dims[dim] // shards_of).reshape((-1,) + (1,) * (len(dims) - dim - 1))

    level = one(*cuts[0])
    for cut in cuts[1:]:
        level = level * one(*cut)
    return level


def shared_out(key, own, number, rows, number_of, top, most, lean):
    sequence = jax.random.permutation(key, number_of)
    crowded, usual = load_shares(number_of, rows * top, most, lean, True), load_shares(number_of, rows * top, most, lean, False)
    places = jnp.arange(number_of)

    def named(tallies, rotation):
        used = int((tallies > 0).sum())
        fixed = max(1, used // 4)
        moved = fixed + (places - fixed + rotation * (used - fixed)) % max(1, number_of - fixed)
        return jnp.zeros((number_of,), jnp.int32).at[sequence[jnp.where(places < fixed, places, moved)]].set(jnp.asarray(tallies, jnp.int32))

    tallies = jnp.where(number % 4 == 0, named(crowded, number // 4), named(usual, number - number // 4 - 1))
    mixed = jax.random.permutation(jax.random.fold_in(own, 3), number_of)
    giver, taker = mixed[0:number_of // 2 * 2:2], mixed[1:number_of // 2 * 2:2]
    slack = jnp.minimum(tallies[giver] - 1, most - tallies[taker]) // 2
    slack = jnp.where((giver == sequence[0]) | (taker == sequence[0]) | (tallies[taker] == 0), 0, jnp.maximum(slack, 0))
    moved = jax.random.randint(jax.random.fold_in(own, 4), (number_of // 2,), 0, 1 << 20) % (slack + 1)
    tallies = tallies.at[giver].add(-moved).at[taker].add(moved)
    labels = jnp.searchsorted(jnp.cumsum(tallies), jnp.arange(rows * top), side="right").astype(jnp.int32)
    listing = labels.reshape(top, rows).T
    listing = listing[jax.random.permutation(jax.random.fold_in(own, 1), rows)]
    rotation = jax.random.randint(jax.random.fold_in(own, 2), (rows, 1), 0, top)
    return jnp.take_along_axis(listing, (jnp.arange(top)[None, :] + rotation) % top, axis=1)


def load_shares(amount, total, reach, skew, full):
    loads = [(1 << 20) // math.isqrt(rank ** skew) + 1 for rank in range(1, amount + 1)]
    largest = reach if full else min(reach, max(-(-total // amount), total * loads[0] // sum(loads)))
    least = 1 if total - largest >= amount - 1 else 0
    counts, spare = [largest] + [least] * (amount - 1), total - largest - least * (amount - 1)
    while spare > 0:
        candidates = [i for i in range(1, amount) if counts[i] < largest] or [i for i in range(1, amount) if counts[i] < reach]
        mass, left = sum([loads[i] for i in candidates]), spare
        for i in candidates:
            addition = min(reach - counts[i], max(1, left * loads[i] // mass), spare)
            counts[i] = counts[i] + addition
            spare = spare - addition
    return np.array(counts)


def normal_values(key, dims, deviation, limit, cuts=(), held_as=jnp.bfloat16):
    values = jax.random.normal(key, dims, jnp.float32) * deviation
    if len(cuts) > 0:
        values = steps_of(key, dims, cuts, -0.22, 0.18) * values
    return jnp.clip(values, min=-limit, max=limit).astype(held_as)


def setup_inputs(seed: int = 0) -> dict:
    seeds = jax.random.split(jax.random.key(seed), 22)
    resid = draw_resid(jax.random.fold_in(seeds[21], 71), 0)
    queries = draw_queries(jax.random.fold_in(seeds[21], 71), 0)
    new_keys = normal_values(seeds[2], (SEQUENCE_TOTAL, KV_HEADS * HEAD), 1.0, 6.0, ((0, 16), (1, 2)))
    new_values = normal_values(seeds[3], (SEQUENCE_TOTAL, KV_HEADS * HEAD), 3.0, 18.0, ((0, 16), (1, 2)))
    key_cache = draw_key_cache(jax.random.fold_in(seeds[21], 71), 0)
    value_cache = normal_values(seeds[5], (SEQUENCE_TOTAL, KV_HEADS, CACHE_SLOTS, HEAD), 3.0, 18.0, ((0, 16), (1, 2)))
    cum_gate = draw_cum_gate(jax.random.fold_in(seeds[21], 71), 0)
    forget_logit = normal_values(seeds[7], (SEQUENCE_TOTAL, QUERY_HEADS), 1.0, 6.0, ((0, 16), (1, 2)), jnp.float32)
    forget_bias = jnp.clip(-3.0 + 5.0 * jax.random.uniform(seeds[8], (QUERY_HEADS,), jnp.float32) ** steps_of(seeds[8], (QUERY_HEADS,), ((0, 2),), -0.2, 0.2), -3.0, 2.0)
    lengths = touch_ends(jax.random.randint(seeds[9], (SEQUENCE_TOTAL,), CACHE_SLOTS // 8, CACHE_SLOTS + 1), jax.random.fold_in(seeds[9], 1), CACHE_SLOTS // 8, CACHE_SLOTS).astype(jnp.int32)
    out_weight = normal_values(seeds[10], (QUERY_HEADS * HEAD, D), (QUERY_HEADS * HEAD) ** -0.5, 0.1875, ((0, 2),))
    norm_gain = jnp.clip(1.0 + 0.18 * jax.random.normal(seeds[11], (D,), jnp.float32), 0.1, 1.9)
    mix_vector = normal_values(seeds[12], (D,), D ** -0.5, 0.125)
    routes_keys = jax.random.split(jax.random.fold_in(seeds[13], 1), SEQUENCE_TOTAL // SEQ_DEV)
    routes_turns = jax.random.permutation(jax.random.fold_in(seeds[13], 3), SEQUENCE_TOTAL // SEQ_DEV)
    routes = jax.vmap(lambda own, number: shared_out(jax.random.fold_in(seeds[13], 2), own, number, SEQ_DEV, EXPERTS, TOP_K, CAP, 1))(routes_keys, routes_turns).reshape((SEQUENCE_TOTAL, TOP_K))
    route_weight = jnp.clip(0.2 + 0.8 * jax.random.uniform(seeds[14], (SEQUENCE_TOTAL, TOP_K), jnp.float32) ** steps_of(seeds[14], (SEQUENCE_TOTAL, TOP_K), ((0, 16),), -0.2, 0.2), 0.2, 1.0)
    expert_gate = normal_values(seeds[15], (N_EP, D, FF_SPAN), D ** -0.5, 0.125, ((0, 16), (1, 2)))
    expert_up = normal_values(seeds[16], (N_EP, D, FF_SPAN), D ** -0.5, 0.125, ((0, 16), (1, 2)))
    expert_down = normal_values(seeds[17], (N_EP, FF_SPAN, D), FF ** -0.5, 0.109375, ((0, 16), (2, 2)))
    dense_gate = normal_values(seeds[18], (D, FFD), D ** -0.5, 0.125, ((0, 2), (1, 16)))
    dense_up = normal_values(seeds[19], (D, FFD), D ** -0.5, 0.125, ((0, 2), (1, 16)))
    dense_down = normal_values(seeds[20], (FFD, D), FFD ** -0.5, 0.109375, ((0, 16), (1, 2)))
    return dict(resid=resid, queries=queries, new_keys=new_keys, new_values=new_values, key_cache=key_cache, value_cache=value_cache, cum_gate=cum_gate, forget_logit=forget_logit, forget_bias=forget_bias, lengths=lengths, out_weight=out_weight, norm_gain=norm_gain, mix_vector=mix_vector, routes=routes, route_weight=route_weight, expert_gate=expert_gate, expert_up=expert_up, expert_down=expert_down, dense_gate=dense_gate, dense_up=dense_up, dense_down=dense_down)


EPSILON = 1e-06

def slot_table(route_block, expert_ids, capacity):
    blocks = route_block.shape[0]
    flat_routes = route_block.reshape(blocks, 1, -1)
    matched = (flat_routes == expert_ids.reshape(1, -1, 1)).astype(jnp.int32)
    ranking = jnp.cumsum(matched, axis=2) - 1
    slot_ids = jnp.arange(capacity, dtype=jnp.int32)
    taken = (matched[..., None] > 0) & (ranking[..., None] == slot_ids)
    table = jnp.swapaxes(taken, 2, 3).astype(jnp.float32)
    return table.reshape(blocks, expert_ids.shape[0], capacity, route_block.shape[1], route_block.shape[2])

def attend(queries, new_keys, new_values, key_cache, value_cache, cum_gate, forget_logit, forget_bias, lengths):
    seqcount = queries.shape[0]
    kv_local = key_cache.shape[1]
    grouping = QUERY_HEADS // KV_HEADS
    heads_local = kv_local * grouping
    scale_factor = 1.0 / math.sqrt(HEAD)
    query_float = queries.astype(jnp.float32).reshape(seqcount, kv_local, grouping, HEAD)
    scores = jnp.einsum('sgjd,sgpd->sgjp', query_float, key_cache.astype(jnp.float32))
    scores = scores.reshape(seqcount, heads_local, -1) * scale_factor
    own_score = jnp.einsum('sgjd,sgd->sgj', query_float, new_keys.astype(jnp.float32).reshape(seqcount, kv_local, HEAD))
    own_score = own_score.reshape(seqcount, heads_local) * scale_factor
    log_forget = jax.nn.log_sigmoid(forget_logit + forget_bias)
    position = jnp.arange(cum_gate.shape[2], dtype=jnp.int32)
    latest = lax.optimization_barrier(jnp.sum(jnp.where(position == (lengths - 1)[:, None, None], cum_gate, 0.0), axis=2))
    scores = scores + (latest + log_forget)[:, :, None] - cum_gate
    visible = position[None, None, :] < lengths[:, None, None]
    scores = jnp.where(visible, scores, -jnp.inf)
    highest = jnp.maximum(lax.optimization_barrier(jnp.max(scores, axis=2)), own_score)
    weights_past = jnp.exp(scores - highest[:, :, None])
    weight_own = jnp.exp(own_score - highest)
    totals = lax.optimization_barrier(jnp.sum(weights_past, axis=2)) + weight_own
    probs_past = (weights_past / totals[:, :, None]).astype(jnp.bfloat16)
    prob_own = (weight_own / totals).astype(jnp.bfloat16)
    mixed = jnp.einsum('sgjp,sgpd->sgjd', probs_past.astype(jnp.float32).reshape(seqcount, kv_local, grouping, -1), value_cache.astype(jnp.float32))
    mixed = mixed + prob_own.astype(jnp.float32).reshape(seqcount, kv_local, grouping, 1) * new_values.astype(jnp.float32).reshape(seqcount, kv_local, 1, HEAD)
    return mixed.reshape(seqcount, heads_local * HEAD).astype(jnp.bfloat16)

def reference(resid, queries, new_keys, new_values, key_cache, value_cache, cum_gate, forget_logit, forget_bias, lengths, out_weight, norm_gain, mix_vector, routes, route_weight, expert_gate, expert_up, expert_down, dense_gate, dense_up, dense_down):

    def per_block(pieces):
        q_block, k_new, v_new, k_cache, v_cache, gates_block, logit_block, length_block = pieces
        return attend(q_block, k_new, v_new, k_cache, v_cache, gates_block, logit_block, forget_bias, length_block)
    pieces = (queries.reshape(N_EP, SEQ_DEV, -1), new_keys.reshape(N_EP, SEQ_DEV, -1), new_values.reshape(N_EP, SEQ_DEV, -1), key_cache.reshape(N_EP, SEQ_DEV, KV_HEADS, CACHE_SLOTS, HEAD), value_cache.reshape(N_EP, SEQ_DEV, KV_HEADS, CACHE_SLOTS, HEAD), cum_gate.reshape(N_EP, SEQ_DEV, QUERY_HEADS, CACHE_SLOTS), forget_logit.reshape(N_EP, SEQ_DEV, QUERY_HEADS), lengths.reshape(N_EP, SEQ_DEV))
    attended = lax.map(per_block, pieces).reshape(SEQUENCE_TOTAL, QUERY_HEADS * HEAD)
    projected = jnp.dot(attended, out_weight, preferred_element_type=jnp.float32).astype(jnp.bfloat16)
    state = resid.astype(jnp.float32) + projected.astype(jnp.float32)
    inverse = lax.rsqrt(lax.optimization_barrier(jnp.mean(state * state, axis=1)) + EPSILON)
    normed = (state * inverse[:, None] * norm_gain).astype(jnp.bfloat16)
    gate = jax.nn.sigmoid(inverse * lax.optimization_barrier(jnp.sum(state * norm_gain * mix_vector.astype(jnp.float32), axis=1)))
    dense_g = jnp.dot(normed, dense_gate, preferred_element_type=jnp.float32)
    dense_u = jnp.dot(normed, dense_up, preferred_element_type=jnp.float32)
    dense_hidden = (jax.nn.silu(dense_g) * dense_u).astype(jnp.bfloat16)
    dense = jnp.dot(dense_hidden, dense_down, preferred_element_type=jnp.float32)
    route_block = routes.reshape(N_EP, SEQ_DEV, TOP_K)
    weight_block = route_weight.reshape(N_EP, SEQ_DEV, TOP_K)
    normed_block = normed.reshape(N_EP, SEQ_DEV, D).astype(jnp.float32)
    gate_blocks = expert_gate.reshape(EXPERTS, EXP_SPAN, D, FF_SPAN)
    up_blocks = expert_up.reshape(EXPERTS, EXP_SPAN, D, FF_SPAN)
    down_blocks = expert_down.reshape(EXPERTS, EXP_SPAN, FF_SPAN, D)

    def expert_step(total, inputs):
        expert_id, gate_part, up_part, down_part = inputs
        w_gate = jnp.transpose(gate_part, (1, 0, 2)).reshape(D, FF)
        w_up = jnp.transpose(up_part, (1, 0, 2)).reshape(D, FF)
        w_down = down_part.reshape(FF, D)
        table = slot_table(route_block, expert_id.reshape(1), CAP)[:, 0]
        picked = lax.optimization_barrier(jnp.sum(table, axis=3))
        chosen = jnp.einsum('bct,btd->bcd', picked, normed_block).astype(jnp.bfloat16).reshape(N_EP * CAP, D)
        gated = jnp.dot(chosen, w_gate, preferred_element_type=jnp.float32)
        upped = jnp.dot(chosen, w_up, preferred_element_type=jnp.float32)
        hidden = (jax.nn.silu(gated) * upped).astype(jnp.bfloat16)
        outputs = jnp.dot(hidden, w_down, preferred_element_type=jnp.float32).reshape(N_EP, CAP, D)
        share = jnp.einsum('bctk,btk,bcd->btd', table, weight_block, outputs, precision=lax.Precision.HIGHEST)
        return (total + share.reshape(SEQUENCE_TOTAL, D), None)
    routed, unused = lax.scan(expert_step, jnp.zeros((SEQUENCE_TOTAL, D), jnp.float32), (jnp.arange(EXPERTS, dtype=jnp.int32), gate_blocks, up_blocks, down_blocks))
    result = state + routed + gate[:, None] * dense
    return result.astype(jnp.bfloat16)
```

```python
import functools
import math

import jax
import jax.numpy as jnp
from jax import lax
from jax.experimental import pallas as pl
from jax.experimental.pallas import tpu as pltpu
from jax.sharding import PartitionSpec as P

HEAD = 128
TOP_K = 2
EXP_SPAN = 4


EPSILON = 1e-06
MESH = pl.DeviceIdType.MESH
META = 128
SEG = 42
GROUPS = 8
ORDER = (0, 1, 4, 5, 6, 7, 2, 3)
CACHE_CHUNKS = 4
STEPS = (
    ("fwd", 0),
    ("in", 0),
    ("fwd", 1),
    ("fwd", 2),
    ("in", 1),
    ("fwd", 3),
    ("in", 2),
    ("mid", 0),
    ("fwd", 4),
    ("in", 3),
    ("mid", 1),
    ("fwd", 5),
    ("in", 4),
    ("mid", 2),
    ("fwd", 6),
    ("in", 5),
    ("mid", 3),
    ("out", 1),
    ("fwd", 7),
    ("in", 6),
    ("mid", 4),
    ("out", 2),
    ("in", 7),
    ("mid", 5),
    ("out", 3),
    ("mid", 6),
    ("out", 4),
    ("mid", 7),
    ("out", 5),
    ("out", 6),
    ("out", 7),
    ("out", 0),
)
VMEM_LIMIT = 60 * 1024 * 1024


def layer_kernel(
    dims,
    q_ref,
    nk_ref,
    nv_ref,
    cum_ref,
    flogit_ref,
    fbias_ref,
    len_ref,
    resid_ref,
    gain_ref,
    mix_ref,
    routes_ref,
    rw_ref,
    kc_hbm,
    vc_hbm,
    ow_hbm,
    eg_hbm,
    eu_hbm,
    ed_hbm,
    dg_hbm,
    du_hbm,
    dd_hbm,
    out_ref,
    kc,
    vc,
    q_buf,
    nk_buf,
    nv_buf,
    lf_buf,
    len_buf,
    score_buf,
    mix_buf,
    att_buf,
    ow,
    eg,
    eu,
    ed,
    dg,
    du,
    dd,
    pp_send,
    pp_recv,
    state_buf,
    norm_buf,
    gat,
    pf,
    psend,
    precv,
    hid,
    rs_send,
    rs_recv,
    load_sem,
    cache_sem,
    pp_ssem,
    pp_rsem,
    ag_ssem,
    ag_psem,
    fwd_ssem,
    ag_rsem,
    p_ssem,
    p_rsem,
    h_ssem,
    h_rsem,
    rs_ssem,
    rs_rsem,
):
    ep_n, tp_n, groups, order = dims
    ep = lax.axis_index("ep")
    tp = lax.axis_index("tp")
    f32, bf16 = jnp.float32, jnp.bfloat16
    tokens, width = out_ref.shape
    span = eg.shape[1]
    dspan = dg.shape[0]
    chips = ep_n // 2
    cpg = chips // groups
    epg = ep_n // groups
    rows = epg * tokens
    part = rows // tp_n
    chip = ep // 2
    core = lax.rem(ep, 2)
    partner = chip * 2 + 1 - core
    mygroup = chip // cpg
    inchip = lax.rem(chip, cpg)

    def place(j):
        return mygroup ^ j

    kv_local = kc.shape[1]
    heads = q_buf.shape[1]
    slots = kc.shape[2]
    grouping = heads // kv_local
    step = tokens // CACHE_CHUNKS
    cache = []
    for side, (src, dst) in enumerate(((kc_hbm, kc), (vc_hbm, vc))):
        for n in range(CACHE_CHUNKS):
            some = pl.ds(n * step, step)
            cache.append(
                pltpu.make_async_copy(src.at[some], dst.at[some], cache_sem.at[side, n])
            )
    for load in cache:
        load.start()
    loads = [
        pltpu.make_async_copy(src, dst, load_sem.at[i])
        for i, (src, dst) in enumerate(
            [
                (ow_hbm, ow),
                (eg_hbm.at[0], eg),
                (eu_hbm.at[0], eu),
                (dg_hbm, dg),
                (du_hbm, du),
                (ed_hbm.at[0], ed),
                (dd_hbm, dd),
            ]
        )
    ]
    loads[0].start()

    barrier = pltpu.get_barrier_semaphore()
    for k in range(1, ep_n):
        pl.semaphore_signal(
            barrier, inc=1, device_id=(lax.rem(ep + k, ep_n), tp), device_id_type=MESH
        )
    for k in range(1, tp_n):
        pl.semaphore_signal(
            barrier, inc=1, device_id=(ep, lax.rem(tp + k, tp_n)), device_id_type=MESH
        )

    eye = lax.broadcasted_iota(jnp.int32, (tokens, tokens), 0) == lax.broadcasted_iota(
        jnp.int32, (tokens, tokens), 1
    )

    def column(row):
        return jnp.sum(jnp.where(eye, row, 0.0), axis=1, keepdims=True)

    for h in range(heads):
        g = h // grouping
        q_buf[:, h, :] = q_ref[:, h * HEAD : (h + 1) * HEAD].astype(f32)
        nk_buf[:, h, :] = nk_ref[:, g * HEAD : (g + 1) * HEAD].astype(f32)
        nv_buf[:, h, :] = nv_ref[:, g * HEAD : (g + 1) * HEAD].astype(f32)
        x = column(flogit_ref[h : h + 1, :]) + fbias_ref[h]
        lf_buf[:, h, :] = jnp.broadcast_to(
            jnp.minimum(x, 0.0) - jnp.log1p(jnp.exp(-jnp.abs(x))), (tokens, HEAD)
        )
    head_row = lax.broadcasted_iota(jnp.int32, (heads, slots), 0)

    def owns(g):
        return (head_row >= g * grouping) & (head_row < (g + 1) * grouping)

    for n in range(tokens):
        if n % step == 0:
            cache[n // step].wait()
        len_buf[n] = jnp.full((heads, HEAD), len_ref[n], jnp.int32)
        every = lax.dot_general(
            q_buf[n].astype(bf16),
            kc[n].reshape(kv_local * slots, HEAD),
            (((1,), (1,)), ((), ())),
            preferred_element_type=f32,
        )
        picked = every[:, 0:slots]
        for g in range(1, kv_local):
            picked = jnp.where(owns(g), every[:, g * slots : (g + 1) * slots], picked)
        score_buf[n] = picked
    for load in loads[1:]:
        load.start()
    scale = 1.0 / math.sqrt(HEAD)
    own = jnp.sum(q_buf[...] * nk_buf[...], axis=2, keepdims=True) * scale
    cum = cum_ref[...]
    length = len_buf[:, :, 0:1]
    position = lax.broadcasted_iota(jnp.int32, (tokens, heads, slots), 2)
    latest = jnp.sum(jnp.where(position == length - 1, cum, 0.0), axis=2, keepdims=True)
    scores = score_buf[...] * scale + (latest + lf_buf[:, :, 0:1]) - cum
    scores = jnp.where(position < length, scores, -jnp.inf)
    highest = jnp.maximum(jnp.max(scores, axis=2, keepdims=True), own)
    past = jnp.exp(scores - highest)
    mine_own = jnp.exp(own - highest)
    totals = jnp.sum(past, axis=2, keepdims=True) + mine_own
    score_buf[...] = past / totals
    own_prob = (mine_own / totals).astype(bf16).astype(f32)
    for n in range(tokens):
        if n % step == 0:
            cache[CACHE_CHUNKS + n // step].wait()
        probs = score_buf[n]
        spread = jnp.concatenate(
            [jnp.where(owns(g), probs, 0.0) for g in range(kv_local)], axis=1
        ).astype(bf16)
        mix_buf[n] = jnp.dot(
            spread, vc[n].reshape(kv_local * slots, HEAD), preferred_element_type=f32
        )
    mix_buf[...] = mix_buf[...] + own_prob * nv_buf[...]
    for h in range(heads):
        att_buf[:, h * HEAD : (h + 1) * HEAD] = mix_buf[:, h, :].astype(bf16)

    loads[0].wait()
    head_part = jnp.dot(att_buf[...], ow[...], preferred_element_type=f32)
    pp_send[...] = head_part.astype(bf16)
    pl.semaphore_wait(barrier, ep_n - 1 + tp_n - 1)

    def remote(src, dst, ssem, rsem, to):
        return pltpu.make_async_remote_copy(
            src_ref=src,
            dst_ref=dst,
            send_sem=ssem,
            recv_sem=rsem,
            device_id=to,
            device_id_type=MESH,
        )

    sends = []
    pp = []
    for k in range(1, tp_n):
        c = remote(
            pp_send,
            pp_recv.at[k - 1],
            pp_ssem.at[k - 1],
            pp_rsem.at[k - 1],
            (ep, lax.rem(tp + k, tp_n)),
        )
        c.start()
        pp.append(c)
        sends.append(c)
    for c in pp:
        c.wait_recv()
    projected = head_part
    for k in range(tp_n - 1):
        projected = projected + pp_recv[k].astype(f32)
    state_full = resid_ref[...].astype(f32) + projected.astype(bf16).astype(f32)
    inverse = lax.rsqrt(jnp.mean(state_full * state_full, axis=1, keepdims=True) + EPSILON)
    scaled_full = state_full * gain_ref[...]
    mix = mix_ref[...].astype(f32)
    mixed = jnp.zeros((tokens, HEAD), f32)
    for n in range(mix.shape[0]):
        mixed = mixed + scaled_full[:, n * HEAD : (n + 1) * HEAD] * mix[n : n + 1, :]
    gate = jax.nn.sigmoid(inverse * jnp.sum(mixed, axis=1, keepdims=True))
    state_buf[...] = state_full
    norm_buf[...] = scaled_full * inverse
    cols = pl.ds(pl.multiple_of(tp * width, 128), width)
    gat[ep, :, 0:width] = norm_buf[:, cols].astype(bf16)
    lane = lax.broadcasted_iota(jnp.int32, (tokens, META), 1)
    named = [column(routes_ref[k : k + 1, :].astype(f32)) for k in range(TOP_K)]
    weighed = [column(rw_ref[k : k + 1, :]) for k in range(TOP_K)]
    meta = jnp.zeros((tokens, META), f32)
    for s in range(3):
        base = s * SEG
        value = jnp.where(lane == base, gate, 0.0)
        for k in range(TOP_K):
            value = value + jnp.where(
                (lane - base - 1).astype(f32) == named[k], weighed[k], 0.0
            )
        value = jnp.where((lane >= base) & (lane < base + SEG), value, 0.0)
        for cut in range(s):
            value = value - value.astype(bf16).astype(f32)
        meta = meta + value
    gat[ep, :, width : width + META] = meta.astype(bf16)

    c = remote(gat.at[ep], gat.at[ep], ag_psem.at[0], ag_rsem.at[ep], (partner, tp))
    c.start()
    sends.append(c)
    for i, j in enumerate(order):
        group = place(j)
        for b in range(cpg):
            if j == 0 and b == 0:
                continue
            target = (group * cpg + lax.rem(inchip + b, cpg)) * 2 + core
            c = remote(
                gat.at[ep], gat.at[ep], ag_ssem.at[i * cpg + b], ag_rsem.at[ep], (target, tp)
            )
            c.start()
            sends.append(c)

    def arrive(src):
        remote(gat.at[src], gat.at[src], ag_psem.at[0], ag_rsem.at[src], (partner, tp)).wait_recv()

    def forward(i):
        j = order[i]
        group = place(j)
        for b in range(cpg):
            if j == 0 and b == 0:
                continue
            src = (group * cpg + lax.rem(inchip + b, cpg)) * 2 + core
            arrive(src)
            c = remote(
                gat.at[src], gat.at[src], fwd_ssem.at[i * cpg + b], ag_rsem.at[src], (partner, tp)
            )
            c.start()
            sends.append(c)

    pcopies = {}
    hcopies = {}
    late = [loads[5], loads[6]]

    def stage_in(i):
        j = order[i]
        group = place(j)
        for b in range(cpg):
            arrive((group * cpg + lax.rem(inchip + b, cpg)) * 2 + 1 - core)
        x = gat[pl.ds(group * epg, epg), :, 0:width].reshape(rows, width)
        at = 0
        for n, w in enumerate((eg, eu, dg, du)):
            if i == 0:
                loads[1 + n].wait()
            if n < 2:
                size = w.shape[1]
                value = jnp.dot(x, w[...], preferred_element_type=f32)
            else:
                size = w.shape[0]
                value = lax.dot_general(
                    x, w[...], (((1,), (1,)), ((), ())), preferred_element_type=f32
                )
            pf[i, :, at : at + size] = value
            psend[i, :, at : at + size] = value.astype(bf16)
            at += size
        pcopies[i] = []
        for k in range(1, tp_n):
            to = lax.rem(tp + k, tp_n)
            c = remote(
                psend.at[i, pl.ds(pl.multiple_of(to * part, 16), part)],
                precv.at[i, k - 1],
                p_ssem.at[i, k - 1],
                p_rsem.at[i, k - 1],
                (ep, to),
            )
            c.start()
            sends.append(c)
            pcopies[i].append(c)

    def stage_mid(i):
        for c in pcopies[i]:
            c.wait_recv()
        mine = pl.ds(pl.multiple_of(tp * part, 16), part)

        def total(at, size):
            value = pf[i, mine, at : at + size]
            for k in range(tp_n - 1):
                value = value + precv[i, k, :, at : at + size].astype(f32)
            return value

        hid[i, mine, 0:span] = (jax.nn.silu(total(0, span)) * total(span, span)).astype(bf16)
        hid[i, mine, span : span + dspan] = (
            jax.nn.silu(total(2 * span, dspan)) * total(2 * span + dspan, dspan)
        ).astype(bf16)
        hcopies[i] = []
        for k in range(1, tp_n):
            to = lax.rem(tp + k, tp_n)
            c = remote(
                hid.at[i, mine],
                hid.at[i, mine],
                h_ssem.at[i, k - 1],
                h_rsem.at[i, k - 1],
                (ep, to),
            )
            c.start()
            sends.append(c)
            source = lax.rem(tp + tp_n - k, tp_n)
            theirs = pl.ds(pl.multiple_of(source * part, 16), part)
            hcopies[i].append(
                remote(
                    hid.at[i, theirs],
                    hid.at[i, theirs],
                    h_ssem.at[i, k - 1],
                    h_rsem.at[i, k - 1],
                    (ep, to),
                )
            )

    expert = ep // EXP_SPAN
    lanes = lax.broadcasted_iota(jnp.int32, (rows, META), 1)

    def stage_out(i):
        j = order[i]
        group = place(j)
        for c in hcopies[i]:
            c.wait_recv()
        while late:
            late.pop().wait()
        info = gat[pl.ds(group * epg, epg), :, width : width + META].reshape(rows, META)
        info = info.astype(f32)
        gates = jnp.sum(
            jnp.where((lanes == 0) | (lanes == SEG) | (lanes == 2 * SEG), info, 0.0),
            axis=1,
            keepdims=True,
        )
        spot = lanes - expert - 1
        shares = jnp.sum(
            jnp.where((spot == 0) | (spot == SEG) | (spot == 2 * SEG), info, 0.0),
            axis=1,
            keepdims=True,
        )
        value = shares * jnp.dot(hid[i, :, 0:span], ed[...], preferred_element_type=f32)
        value = value + gates * jnp.dot(
            hid[i, :, span : span + dspan], dd[...], preferred_element_type=f32
        )
        rs_send[i] = value.astype(bf16).reshape(epg, tokens, width)
        member = lax.rem(ep, epg)
        for b in range(epg):
            slot = lax.rem(member + b, epg)
            if j == 0 and b == 0:
                rs_recv[ep] = rs_send[i, slot]
                continue
            c = remote(
                rs_send.at[i, slot],
                rs_recv.at[ep],
                rs_ssem.at[i * epg + b],
                rs_rsem.at[ep],
                (group * epg + slot, tp),
            )
            c.start()
            sends.append(c)

    stages = {"in": stage_in, "fwd": forward, "mid": stage_mid, "out": stage_out}
    steps = STEPS
    if groups == 1:
        steps = (("fwd", 0), ("in", 0), ("mid", 0), ("out", 0))
    for stage, i in steps:
        stages[stage](i)

    for k in range(1, ep_n):
        src = lax.rem(ep + k, ep_n)
        remote(
            rs_recv.at[src], rs_recv.at[src], rs_ssem.at[0], rs_rsem.at[src], (partner, tp)
        ).wait_recv()
    result = state_buf[:, cols] + jnp.sum(rs_recv[...].astype(f32), axis=0)
    out_ref[...] = result.astype(bf16)
    for c in sends:
        c.wait_send()


def layer_call(
    q, nk, nv, cum, flogit, fbias, lengths, resid, gain, mix, routes, route_weight, kc, vc, ow, eg,
    eu, ed, dg, du, dd,
):
    ep_n, tp_n = lax.axis_size("ep"), lax.axis_size("tp")
    groups = GROUPS if (ep_n // 2) % GROUPS == 0 else 1
    order = ORDER if groups == GROUPS else (0,)
    tokens, full = resid.shape
    width = full // tp_n
    epg = ep_n // groups
    rows = epg * tokens
    part = rows // tp_n
    span, dspan = eg.shape[2], dg.shape[0]
    hidden = span + dspan
    assert ep_n // EXP_SPAN + 1 <= SEG
    f32, bf16 = jnp.float32, jnp.bfloat16
    heads = cum.shape[1]
    smem = pl.BlockSpec(memory_space=pltpu.SMEM)
    vmem = pl.BlockSpec(memory_space=pltpu.VMEM)
    hbm = pl.BlockSpec(memory_space=pl.ANY)
    dma = pltpu.SemaphoreType.DMA
    peers = max(tp_n - 1, 1)
    return pl.pallas_call(
        functools.partial(layer_kernel, (ep_n, tp_n, groups, order)),
        out_shape=pltpu.VMEM((tokens, width), bf16),
        in_specs=[vmem] * 5 + [smem] * 2 + [vmem] * 5 + [hbm] * 9,
        out_specs=vmem,
        scratch_shapes=[
            pltpu.VMEM(kc.shape, bf16),
            pltpu.VMEM(vc.shape, bf16),
            pltpu.VMEM((tokens, heads, HEAD), f32),
            pltpu.VMEM((tokens, heads, HEAD), f32),
            pltpu.VMEM((tokens, heads, HEAD), f32),
            pltpu.VMEM((tokens, heads, HEAD), f32),
            pltpu.VMEM((tokens, heads, HEAD), jnp.int32),
            pltpu.VMEM(cum.shape, f32),
            pltpu.VMEM((tokens, heads, HEAD), f32),
            pltpu.VMEM((tokens, heads * HEAD), bf16),
            pltpu.VMEM(ow.shape, bf16),
            pltpu.VMEM(eg.shape[1:], bf16),
            pltpu.VMEM(eu.shape[1:], bf16),
            pltpu.VMEM(ed.shape[1:], bf16),
            pltpu.VMEM(dg.shape, bf16),
            pltpu.VMEM(du.shape, bf16),
            pltpu.VMEM(dd.shape, bf16),
            pltpu.VMEM((tokens, full), bf16),
            pltpu.VMEM((peers, tokens, full), bf16),
            pltpu.VMEM((tokens, full), f32),
            pltpu.VMEM((tokens, full), f32),
            pltpu.VMEM((ep_n, tokens, width + META), bf16),
            pltpu.VMEM((groups, rows, 2 * hidden), f32),
            pltpu.VMEM((groups, rows, 2 * hidden), bf16),
            pltpu.VMEM((groups, peers, part, 2 * hidden), bf16),
            pltpu.VMEM((groups, rows, hidden), bf16),
            pltpu.VMEM((groups, epg, tokens, width), bf16),
            pltpu.VMEM((ep_n, tokens, width), bf16),
            dma((7,)),
            dma((2, CACHE_CHUNKS)),
            dma((peers,)),
            dma((peers,)),
            dma((ep_n // 2,)),
            dma((1,)),
            dma((ep_n // 2,)),
            dma((ep_n,)),
            dma((groups, peers)),
            dma((groups, peers)),
            dma((groups, peers)),
            dma((groups, peers)),
            dma((ep_n,)),
            dma((ep_n,)),
        ],
        compiler_params=pltpu.CompilerParams(
            collective_id=0, has_side_effects=True, vmem_limit_bytes=VMEM_LIMIT
        ),
        name="layer",
    )(
        q, nk, nv, cum, flogit, fbias, lengths, resid, gain, mix, routes, route_weight, kc, vc, ow,
        eg, eu, ed, dg, du, dd,
    )


def body(
    resid,
    queries,
    new_keys,
    new_values,
    key_cache,
    value_cache,
    cum_gate,
    forget_logit,
    forget_bias,
    lengths,
    out_weight,
    norm_gain,
    mix_vector,
    routes,
    route_weight,
    expert_gate,
    expert_up,
    expert_down,
    dense_gate,
    dense_up,
    dense_down,
):
    result = layer_call(
        queries,
        new_keys,
        new_values,
        cum_gate,
        forget_logit.T,
        forget_bias,
        lengths,
        resid,
        norm_gain.reshape(1, -1),
        mix_vector.reshape(-1, HEAD),
        routes.T,
        route_weight.T,
        key_cache,
        value_cache,
        out_weight,
        expert_gate,
        expert_up,
        expert_down,
        dense_gate.T,
        dense_up.T,
        dense_down,
    )
    return result


def solution(mesh):
    placed = (
        P("ep", None),
        P("ep", "tp"),
        P("ep", "tp"),
        P("ep", "tp"),
        P("ep", "tp", None, None),
        P("ep", "tp", None, None),
        P("ep", "tp", None),
        P("ep", "tp"),
        P("tp"),
        P("ep"),
        P("tp", None),
        P(),
        P(),
        P("ep", None),
        P("ep", None),
        P("ep", "tp", None),
        P("ep", "tp", None),
        P("ep", None, "tp"),
        P("tp", "ep"),
        P("tp", "ep"),
        P("ep", "tp"),
    )
    return jax.shard_map(body, mesh=mesh, in_specs=placed, out_specs=P("ep", "tp"), check_vma=False)
```

```python
import functools
import math

import jax
import jax.numpy as jnp
from jax import lax
from jax.experimental import pallas as pl
from jax.experimental.pallas import tpu as pltpu
from jax.sharding import PartitionSpec as P

HEAD = 128
TOP_K = 2
EXP_SPAN = 4


EPSILON = 1e-06
MESH = pl.DeviceIdType.MESH
META = 128
SEG = 42
PLANES = 4
FAR = (1, 2, 3)
STEPS = (
    ("fwd", 0),
    ("in", 0),
    ("in", 1),
    ("fwd", 2),
    ("in", 2),
    ("fwd", 3),
    ("mid", 1),
    ("in", 3),
    ("fwd", 4),
    ("mid", 2),
    ("in", 4),
    ("mid", 0),
    ("out", 1),
    ("red", 1),
    ("mid", 3),
    ("out", 0),
    ("red", 0),
    ("out", 2),
    ("mid", 4),
    ("red", 2),
    ("out", 3),
    ("red", 3),
    ("out", 4),
    ("red", 4),
)
CACHE_CHUNKS = 4
VMEM_LIMIT = 60 * 1024 * 1024


def layer_kernel(
    dims,
    q_hbm,
    nk_hbm,
    nv_hbm,
    cum_hbm,
    flogit_hbm,
    fbias_hbm,
    len_hbm,
    resid_hbm,
    gain_hbm,
    mix_hbm,
    routes_hbm,
    rw_hbm,
    kc_hbm,
    vc_hbm,
    ow_hbm,
    eg_hbm,
    eu_hbm,
    ed_hbm,
    dg_hbm,
    du_hbm,
    dd_hbm,
    out_ref,
    q_ref,
    nk_ref,
    nv_ref,
    cum_ref,
    flogit_ref,
    fbias_ref,
    len_ref,
    resid_ref,
    gain_ref,
    mix_ref,
    routes_ref,
    rw_ref,
    kc,
    vc,
    q_buf,
    nk_buf,
    nv_buf,
    lf_buf,
    len_buf,
    add_buf,
    score_buf,
    mix_buf,
    att_buf,
    ow,
    wgu,
    wd,
    dgu,
    pp_send,
    pp_recv,
    state_buf,
    norm_buf,
    gat,
    pf,
    psend,
    precv,
    aff,
    asend,
    arecv,
    hid,
    outs,
    cs_send,
    cs_recv,
    rs_send,
    rs_recv,
    small_sem,
    load_sem,
    cache_sem,
    pp_ssem,
    pp_rsem,
    ag_ssem,
    ag_psem,
    ag_rsem,
    p_ssem,
    p_rsem,
    h_ssem,
    h_rsem,
    c_ssem,
    c_rsem,
    rs_ssem,
    rs_rsem,
):
    ep_n, tp_n, sets = dims
    ep = lax.axis_index("ep")
    tp = lax.axis_index("tp")
    f32, bf16 = jnp.float32, jnp.bfloat16
    tokens, width = out_ref.shape
    span = eg_hbm.shape[2]
    dspan = dg_hbm.shape[0]
    hidden = span + dspan
    chips = ep_n // 2
    chip = ep // 2
    core = lax.rem(ep, 2)
    partner = chip * 2 + 1 - core
    sizes = [2 * count * tokens for count, where, direct, whole in sets]
    firsts = [sum(sizes[:i]) for i in range(len(sets))]

    kv_local = kc.shape[1]
    heads = q_buf.shape[1]
    slots = kc.shape[2]
    grouping = heads // kv_local
    step = tokens // CACHE_CHUNKS
    cache = []
    for side, (src, dst) in enumerate(((kc_hbm, kc), (vc_hbm, vc))):
        for n in range(CACHE_CHUNKS):
            some = pl.ds(n * step, step)
            cache.append(
                pltpu.make_async_copy(src.at[some], dst.at[some], cache_sem.at[side, n])
            )
    smalls = [
        pltpu.make_async_copy(src, dst, small_sem.at[i])
        for i, (src, dst) in enumerate(
            [
                (q_hbm, q_ref),
                (nk_hbm, nk_ref),
                (nv_hbm, nv_ref),
                (flogit_hbm, flogit_ref),
                (fbias_hbm, fbias_ref),
                (len_hbm, len_ref),
                (cum_hbm, cum_ref),
                (resid_hbm, resid_ref),
                (gain_hbm, gain_ref),
                (mix_hbm, mix_ref),
                (routes_hbm, routes_ref),
                (rw_hbm, rw_ref),
            ]
        )
    ]
    smalls[0].start()
    cache[0].start()
    for load in smalls[1:7]:
        load.start()
    for load in cache[1:]:
        load.start()
    loads = [
        pltpu.make_async_copy(src, dst, load_sem.at[i])
        for i, (src, dst) in enumerate(
            [
                (ow_hbm, ow),
                (dg_hbm, dgu.at[0:dspan]),
                (du_hbm, dgu.at[dspan : 2 * dspan]),
                (eg_hbm.at[0], wgu.at[:, 0:span]),
                (eu_hbm.at[0], wgu.at[:, span : 2 * span]),
                (ed_hbm.at[0], wd.at[0:span]),
                (dd_hbm, wd.at[span:hidden]),
            ]
        )
    ]
    loads[0].start()
    for load in smalls[7:]:
        load.start()

    barrier = pltpu.get_barrier_semaphore()
    for k in range(1, ep_n):
        pl.semaphore_signal(
            barrier, inc=1, device_id=(lax.rem(ep + k, ep_n), tp), device_id_type=MESH
        )
    for k in range(1, tp_n):
        pl.semaphore_signal(
            barrier, inc=1, device_id=(ep, lax.rem(tp + k, tp_n)), device_id_type=MESH
        )

    eye = lax.broadcasted_iota(jnp.int32, (tokens, tokens), 0) == lax.broadcasted_iota(
        jnp.int32, (tokens, tokens), 1
    )

    def column(row):
        return jnp.sum(jnp.where(eye, row, 0.0), axis=1, keepdims=True)

    q_buf[...] = jnp.zeros_like(q_buf)
    for load in smalls[0:6]:
        load.wait()
    for h in range(heads):
        g = h // grouping
        one = slice(g * HEAD, (g + 1) * HEAD)
        q_buf[:, h, one] = q_ref[:, h * HEAD : (h + 1) * HEAD].astype(f32)
        nk_buf[:, h, :] = nk_ref[...].astype(f32)
        nv_buf[:, h, :] = nv_ref[:, one].astype(f32)
        x = column(flogit_ref[h : h + 1, :]) + fbias_ref[h]
        lf_buf[:, h, :] = jnp.broadcast_to(
            jnp.minimum(x, 0.0) - jnp.log1p(jnp.exp(-jnp.abs(x))), (tokens, HEAD)
        )
    head_row = lax.broadcasted_iota(jnp.int32, (heads, HEAD), 0)
    for n in range(tokens):
        len_buf[n] = jnp.full((heads, HEAD), len_ref[n], jnp.int32)

    def beside(ref, n):
        return jnp.concatenate([ref[n, g] for g in range(kv_local)], axis=1)

    scale = 1.0 / math.sqrt(HEAD)
    own = jnp.sum(q_buf[...] * nk_buf[...], axis=2, keepdims=True) * scale
    smalls[6].wait()
    cum = cum_ref[...]
    length = len_buf[:, :, 0:1]
    position = lax.broadcasted_iota(jnp.int32, (tokens, heads, slots), 2)
    latest = jnp.sum(jnp.where(position == length - 1, cum, 0.0), axis=2, keepdims=True)
    add_buf[...] = jnp.where(
        position < length, (latest + lf_buf[:, :, 0:1]) - cum, -jnp.inf
    )
    for n in range(tokens):
        if n % step == 0:
            cache[n // step].wait()
        score_buf[n] = lax.dot_general(
            q_buf[n].astype(bf16),
            beside(kc, n),
            (((1,), (1,)), ((), ())),
            preferred_element_type=f32,
        )
    for load in loads[1:]:
        load.start()
    scores = score_buf[...] * scale + add_buf[...]
    highest = jnp.maximum(jnp.max(scores, axis=2, keepdims=True), own)
    past = jnp.exp(scores - highest)
    mine_own = jnp.exp(own - highest)
    totals = jnp.sum(past, axis=2, keepdims=True) + mine_own
    score_buf[...] = past / totals
    own_prob = (mine_own / totals).astype(bf16).astype(f32)
    for n in range(tokens):
        if n % step == 0:
            cache[CACHE_CHUNKS + n // step].wait()
        both = jnp.dot(score_buf[n].astype(bf16), beside(vc, n), preferred_element_type=f32)
        taken = both[:, 0:HEAD]
        for g in range(1, kv_local):
            taken = jnp.where(
                head_row >= g * grouping, both[:, g * HEAD : (g + 1) * HEAD], taken
            )
        mix_buf[n] = taken
    mix_buf[...] = mix_buf[...] + own_prob * nv_buf[...]
    for h in range(heads):
        att_buf[:, h * HEAD : (h + 1) * HEAD] = mix_buf[:, h, :].astype(bf16)

    loads[0].wait()
    head_part = jnp.dot(att_buf[...], ow[...], preferred_element_type=f32)
    pp_send[...] = head_part.astype(bf16)
    pl.semaphore_wait(barrier, ep_n - 1 + tp_n - 1)

    def remote(src, dst, ssem, rsem, to):
        return pltpu.make_async_remote_copy(
            src_ref=src,
            dst_ref=dst,
            send_sem=ssem,
            recv_sem=rsem,
            device_id=to,
            device_id_type=MESH,
        )

    sends = []
    pp = []
    for k in range(1, tp_n):
        c = remote(
            pp_send,
            pp_recv.at[k - 1],
            pp_ssem.at[k - 1],
            pp_rsem.at[k - 1],
            (ep, lax.rem(tp + k, tp_n)),
        )
        c.start()
        pp.append(c)
        sends.append(c)
    for load in smalls[7:]:
        load.wait()
    loads[1].wait()
    loads[2].wait()
    wgu[:, 2 * span : 2 * hidden] = dgu[...].T
    for c in pp:
        c.wait_recv()
    projected = head_part
    for k in range(tp_n - 1):
        projected = projected + pp_recv[k].astype(f32)
    state_full = resid_ref[...].astype(f32) + projected.astype(bf16).astype(f32)
    inverse = lax.rsqrt(jnp.mean(state_full * state_full, axis=1, keepdims=True) + EPSILON)
    scaled_full = state_full * gain_ref[...]
    mix = mix_ref[...].astype(f32)
    mixed = jnp.zeros((tokens, HEAD), f32)
    for n in range(mix.shape[0]):
        mixed = mixed + scaled_full[:, n * HEAD : (n + 1) * HEAD] * mix[n : n + 1, :]
    gate = jax.nn.sigmoid(inverse * jnp.sum(mixed, axis=1, keepdims=True))
    state_buf[...] = state_full
    norm_buf[...] = scaled_full * inverse
    cols = pl.ds(pl.multiple_of(tp * width, 128), width)
    gat[core, chip, :, 0:width] = norm_buf[:, cols].astype(bf16)
    lane = lax.broadcasted_iota(jnp.int32, (tokens, META), 1)
    named = [column(routes_ref[k : k + 1, :].astype(f32)) for k in range(TOP_K)]
    weighed = [column(rw_ref[k : k + 1, :]) for k in range(TOP_K)]
    meta = jnp.zeros((tokens, META), f32)
    for s in range(3):
        base = s * SEG
        value = jnp.where(lane == base, gate, 0.0)
        for k in range(TOP_K):
            value = value + jnp.where(
                (lane - base - 1).astype(f32) == named[k], weighed[k], 0.0
            )
        value = jnp.where((lane >= base) & (lane < base + SEG), value, 0.0)
        for cut in range(s):
            value = value - value.astype(bf16).astype(f32)
        meta = meta + value
    gat[core, chip, :, width : width + META] = meta.astype(bf16)

    def put(src, dst, ssem, rsem, to):
        c = remote(src, dst, ssem, rsem, to)
        c.start()
        sends.append(c)
        return c

    block = gat.at[core, chip]
    put(block, block, ag_psem.at[0], ag_rsem.at[core, chip], (partner, tp))

    def others(i):
        count, where, direct, whole = sets[i]
        first = where(chip)
        for b in range(count):
            if whole and b == 0:
                continue
            yield first + lax.rem(chip + b, count) if count > 1 else first

    number = [0]

    def spot():
        number[0] += 1
        return number[0] - 1

    for i in range(len(sets)):
        for there in others(i):
            put(block, block, ag_ssem.at[spot()], ag_rsem.at[core, chip], (there * 2 + core, tp))
            if sets[i][2]:
                put(
                    block,
                    block,
                    ag_ssem.at[spot()],
                    ag_rsem.at[core, chip],
                    (there * 2 + 1 - core, tp),
                )

    def arrive(side, there):
        came = gat.at[side, there]
        remote(came, came, ag_psem.at[0], ag_rsem.at[side, there], (partner, tp)).wait_recv()

    def forward(i):
        for there in others(i):
            arrive(core, there)
            came = gat.at[core, there]
            if not sets[i][2]:
                put(came, came, ag_ssem.at[spot()], ag_rsem.at[core, there], (partner, tp))

    pcopies = {}
    hcopies = {}
    early = loads[3:5]
    late = loads[5:7]

    def piece(i, k):
        count, where, direct, whole = sets[i]
        share = 2 * count // tp_n
        at = k * share
        return gat.at[at // count, pl.ds(where(chip) + lax.rem(at, count), share)]

    def everything(i):
        count, where, direct, whole = sets[i]
        return [gat.at[side, pl.ds(where(chip), count)] for side in range(2)]

    def stage_in(i):
        count, where, direct, whole = sets[i]
        if direct:
            forward(i)
        if whole:
            arrive(1 - core, chip)
        for there in others(i):
            arrive(1 - core, there)
        while early:
            early.pop().wait()
        pcopies[i] = []
        if whole:
            pieces = everything(i)
        else:
            pieces = [piece(i, lax.rem(tp + k, tp_n)) for k in range(tp_n)]
        x = jnp.concatenate(
            [one[:, :, 0:width].reshape(sizes[i] // len(pieces), width) for one in pieces], axis=0
        )
        value = jnp.dot(x, wgu[...], preferred_element_type=f32)
        if whole:
            aff[...] = value
            asend[...] = value.astype(bf16)
        else:
            part = sizes[i] // tp_n
            at = pl.ds(firsts[i] // tp_n, part)
            pf[at] = value[0:part]
        for k in range(1, tp_n):
            if whole:
                src, dst = asend, arecv.at[k - 1]
            else:
                psend[k - 1, at] = value[k * part : (k + 1) * part].astype(bf16)
                src, dst = psend.at[k - 1, at], precv.at[k - 1, at]
            pcopies[i].append(
                put(
                    src,
                    dst,
                    p_ssem.at[i, k - 1],
                    p_rsem.at[i, k - 1],
                    (ep, lax.rem(tp + k, tp_n)),
                )
            )

    expert = ep // EXP_SPAN

    def stage_mid(i):
        for c in pcopies[i]:
            c.wait_recv()
        whole = sets[i][3]
        hcopies[i] = []
        if whole:
            part, pieces = sizes[i], everything(i)
            own, other, at = aff, arecv, pl.ds(0, part)
        else:
            part, pieces = sizes[i] // tp_n, [piece(i, tp)]
            own, other, at = pf, precv, pl.ds(firsts[i] // tp_n, part)

        def total(low, size):
            value = own[at, low : low + size]
            for k in range(tp_n - 1):
                value = value + other[k, at, low : low + size].astype(f32)
            return value

        lanes = lax.broadcasted_iota(jnp.int32, (part, META), 1)
        info = jnp.concatenate(
            [
                one[:, :, width : width + META].reshape(part // len(pieces), META)
                for one in pieces
            ],
            axis=0,
        ).astype(f32)

        def picked(lane):
            spot = lanes - lane
            return jnp.sum(
                jnp.where((spot == 0) | (spot == SEG) | (spot == 2 * SEG), info, 0.0),
                axis=1,
                keepdims=True,
            )

        routed = picked(expert + 1) * jax.nn.silu(total(0, span)) * total(span, span)
        dense = picked(0) * jax.nn.silu(total(2 * span, dspan)) * total(2 * span + dspan, dspan)
        if whole:
            mine = pl.ds(firsts[i], part)
        else:
            mine = pl.ds(pl.multiple_of(firsts[i] + tp * part, 16), part)
        hid[mine, 0:span] = routed.astype(bf16)
        hid[mine, span:hidden] = dense.astype(bf16)
        if whole:
            return
        for k in range(1, tp_n):
            to = lax.rem(tp + k, tp_n)
            put(hid.at[mine], hid.at[mine], h_ssem.at[i, k - 1], h_rsem.at[i, k - 1], (ep, to))
            source = lax.rem(tp + tp_n - k, tp_n)
            theirs = pl.ds(pl.multiple_of(firsts[i] + source * part, 16), part)
            hcopies[i].append(
                remote(
                    hid.at[theirs],
                    hid.at[theirs],
                    h_ssem.at[i, k - 1],
                    h_rsem.at[i, k - 1],
                    (ep, to),
                )
            )

    ccopies = {}

    def stage_out(i):
        for c in hcopies[i]:
            c.wait_recv()
        while late:
            late.pop().wait()
        value = jnp.dot(
            hid[firsts[i] : firsts[i] + sizes[i]], wd[...], preferred_element_type=f32
        )
        half = sizes[i] // 2
        at = pl.ds(firsts[i] // 2, half)
        outs[0, at] = value[0:half]
        outs[1, at] = value[half : 2 * half]
        cs_send[at] = outs[1 - core, at].astype(bf16)
        ccopies[i] = put(
            cs_send.at[at], cs_recv.at[at], c_ssem.at[i], c_rsem.at[i], (partner, tp)
        )

    def stage_red(i):
        count, where, direct, whole = sets[i]
        ccopies[i].wait_recv()
        at = pl.ds(firsts[i] // 2, sizes[i] // 2)
        value = outs[core, at] + cs_recv[at].astype(f32)
        first = firsts[i] // 2 // tokens
        rs_send[pl.ds(first, count)] = value.astype(bf16).reshape(count, tokens, width)
        for b in range(count):
            slot = lax.rem(chip + b, count)
            if whole and b == 0:
                rs_recv[chip] = rs_send[first + slot]
                continue
            put(
                rs_send.at[first + slot],
                rs_recv.at[chip],
                rs_ssem.at[first + b],
                rs_rsem.at[chip],
                ((where(chip) + slot) * 2 + core, tp),
            )

    stages = {
        "in": stage_in,
        "fwd": forward,
        "mid": stage_mid,
        "out": stage_out,
        "red": stage_red,
    }
    steps = STEPS
    if len(sets) == 1:
        steps = (("fwd", 0), ("in", 0), ("mid", 0), ("out", 0), ("red", 0))
    for stage, i in steps:
        stages[stage](i)

    for k in range(1, chips):
        src = lax.rem(chip + k, chips)
        remote(
            rs_recv.at[src], rs_recv.at[src], rs_ssem.at[0], rs_rsem.at[src], (partner, tp)
        ).wait_recv()
    result = state_buf[:, cols] + jnp.sum(rs_recv[...].astype(f32), axis=0)
    out_ref[...] = result.astype(bf16)
    for c in sends:
        c.wait_send()


def plan(chips):
    planes = PLANES
    if chips % (2 * planes):
        return ((chips, lambda chip: 0, False, True),)
    deep = chips // planes
    half = deep // 2

    def other(k):
        return lambda chip: (chip // deep ^ k) * deep

    return (
        (half, lambda chip: chip // half * half, False, True),
        (half, lambda chip: (chip // half ^ 1) * half, True, False),
    ) + tuple((deep, other(k), False, False) for k in FAR)


def layer_call(
    q, nk, nv, cum, flogit, fbias, lengths, resid, gain, mix, routes, route_weight, kc, vc, ow, eg,
    eu, ed, dg, du, dd,
):
    ep_n, tp_n = lax.axis_size("ep"), lax.axis_size("tp")
    chips = ep_n // 2
    sets = plan(chips)
    tokens, full = resid.shape
    width = full // tp_n
    rows = ep_n * tokens
    whole = 2 * sets[0][0] * tokens
    count = len(sets)
    span, dspan = eg.shape[2], dg.shape[0]
    hidden = span + dspan
    assert ep_n // EXP_SPAN + 1 <= SEG
    f32, bf16 = jnp.float32, jnp.bfloat16
    heads = cum.shape[1]
    vmem = pl.BlockSpec(memory_space=pltpu.VMEM)
    hbm = pl.BlockSpec(memory_space=pl.ANY)
    dma = pltpu.SemaphoreType.DMA
    peers = max(tp_n - 1, 1)
    return pl.pallas_call(
        functools.partial(layer_kernel, (ep_n, tp_n, sets)),
        out_shape=pltpu.VMEM((tokens, width), bf16),
        in_specs=[hbm] * 21,
        out_specs=vmem,
        scratch_shapes=[
            pltpu.VMEM(q.shape, bf16),
            pltpu.VMEM(nk.shape, bf16),
            pltpu.VMEM(nv.shape, bf16),
            pltpu.VMEM(cum.shape, f32),
            pltpu.VMEM(flogit.shape, f32),
            pltpu.SMEM(fbias.shape, f32),
            pltpu.SMEM(lengths.shape, jnp.int32),
            pltpu.VMEM(resid.shape, bf16),
            pltpu.VMEM(gain.shape, f32),
            pltpu.VMEM(mix.shape, bf16),
            pltpu.VMEM(routes.shape, jnp.int32),
            pltpu.VMEM(route_weight.shape, f32),
            pltpu.VMEM(kc.shape, bf16),
            pltpu.VMEM(vc.shape, bf16),
            pltpu.VMEM((tokens, heads, nk.shape[1]), f32),
            pltpu.VMEM((tokens, heads, nk.shape[1]), f32),
            pltpu.VMEM((tokens, heads, HEAD), f32),
            pltpu.VMEM((tokens, heads, HEAD), f32),
            pltpu.VMEM((tokens, heads, HEAD), jnp.int32),
            pltpu.VMEM(cum.shape, f32),
            pltpu.VMEM(cum.shape, f32),
            pltpu.VMEM((tokens, heads, HEAD), f32),
            pltpu.VMEM((tokens, heads * HEAD), bf16),
            pltpu.VMEM(ow.shape, bf16),
            pltpu.VMEM((width, 2 * hidden), bf16),
            pltpu.VMEM((hidden, width), bf16),
            pltpu.VMEM((2 * dspan, width), bf16),
            pltpu.VMEM((tokens, full), bf16),
            pltpu.VMEM((peers, tokens, full), bf16),
            pltpu.VMEM((tokens, full), f32),
            pltpu.VMEM((tokens, full), f32),
            pltpu.VMEM((2, chips, tokens, width + META), bf16),
            pltpu.VMEM((rows // tp_n, 2 * hidden), f32),
            pltpu.VMEM((peers, rows // tp_n, 2 * hidden), bf16),
            pltpu.VMEM((peers, rows // tp_n, 2 * hidden), bf16),
            pltpu.VMEM((whole, 2 * hidden), f32),
            pltpu.VMEM((whole, 2 * hidden), bf16),
            pltpu.VMEM((peers, whole, 2 * hidden), bf16),
            pltpu.VMEM((rows, hidden), bf16),
            pltpu.VMEM((2, rows // 2, width), f32),
            pltpu.VMEM((rows // 2, width), bf16),
            pltpu.VMEM((rows // 2, width), bf16),
            pltpu.VMEM((chips, tokens, width), bf16),
            pltpu.VMEM((chips, tokens, width), bf16),
            dma((12,)),
            dma((7,)),
            dma((2, CACHE_CHUNKS)),
            dma((peers,)),
            dma((peers,)),
            dma((3 * chips,)),
            dma((1,)),
            dma((2, chips)),
            dma((count, peers)),
            dma((count, peers)),
            dma((count, peers)),
            dma((count, peers)),
            dma((count,)),
            dma((count,)),
            dma((chips,)),
            dma((chips,)),
        ],
        compiler_params=pltpu.CompilerParams(
            collective_id=0, has_side_effects=True, vmem_limit_bytes=VMEM_LIMIT
        ),
        name="layer",
    )(
        q, nk, nv, cum, flogit, fbias, lengths, resid, gain, mix, routes, route_weight, kc, vc, ow,
        eg, eu, ed, dg, du, dd,
    )


def body(
    resid,
    queries,
    new_keys,
    new_values,
    key_cache,
    value_cache,
    cum_gate,
    forget_logit,
    forget_bias,
    lengths,
    out_weight,
    norm_gain,
    mix_vector,
    routes,
    route_weight,
    expert_gate,
    expert_up,
    expert_down,
    dense_gate,
    dense_up,
    dense_down,
):
    result = layer_call(
        queries,
        new_keys,
        new_values,
        cum_gate,
        forget_logit.T,
        forget_bias,
        lengths,
        resid,
        norm_gain.reshape(1, -1),
        mix_vector.reshape(-1, HEAD),
        routes.T,
        route_weight.T,
        key_cache,
        value_cache,
        out_weight,
        expert_gate,
        expert_up,
        expert_down,
        dense_gate.T,
        dense_up.T,
        dense_down,
    )
    return result


def solution(mesh):
    placed = (
        P("ep", None),
        P("ep", "tp"),
        P("ep", "tp"),
        P("ep", "tp"),
        P("ep", "tp", None, None),
        P("ep", "tp", None, None),
        P("ep", "tp", None),
        P("ep", "tp"),
        P("tp"),
        P("ep"),
        P("tp", None),
        P(),
        P(),
        P("ep", None),
        P("ep", None),
        P("ep", "tp", None),
        P("ep", "tp", None),
        P("ep", None, "tp"),
        P("tp", "ep"),
        P("tp", "ep"),
        P("ep", "tp"),
    )
    return jax.shard_map(body, mesh=mesh, in_specs=placed, out_specs=P("ep", "tp"), check_vma=False)
```

```python
import functools
import math

import jax
import jax.numpy as jnp
from jax import lax
from jax.experimental import pallas as pl
from jax.experimental.pallas import tpu as pltpu
from jax.sharding import PartitionSpec as P

HEAD = 128
TOP_K = 2
EXP_SPAN = 4


EPSILON = 1e-06
MESH = pl.DeviceIdType.MESH
META = 128
SEG = 42
PLANES = 4
ORDER = ((1, 2, 3), (0, 3, 2), (0, 3, 1), (0, 2, 1))
SENDS = ((2, 3, 1), (0, 2, 3), (1, 3, 0), (1, 2, 0))
SPLIT = (2,)
STEPS = (
    ("fwd", 0),
    ("in", 0),
    ("in", 1),
    ("fwd", 2),
    ("in", 2),
    ("fwd", 3),
    ("mid", 1),
    ("in", 3),
    ("fwd", 4),
    ("mid", 2),
    ("in", 4),
    ("fwd", 5),
    ("in", 5),
    ("mid", 0),
    ("out", 1),
    ("red", 1),
    ("mid", 3),
    ("out", 0),
    ("red", 0),
    ("out", 2),
    ("mid", 4),
    ("red", 2),
    ("mid", 5),
    ("out", 3),
    ("red", 3),
    ("out", 4),
    ("red", 4),
    ("out", 5),
    ("red", 5),
)
CACHE_CHUNKS = 4
VMEM_LIMIT = 60 * 1024 * 1024


def layer_kernel(
    dims,
    q_hbm,
    nk_hbm,
    nv_hbm,
    cum_hbm,
    flogit_hbm,
    fbias_hbm,
    len_hbm,
    resid_hbm,
    gain_hbm,
    mix_hbm,
    routes_hbm,
    rw_hbm,
    kc_hbm,
    vc_hbm,
    ow_hbm,
    eg_hbm,
    eu_hbm,
    ed_hbm,
    dg_hbm,
    du_hbm,
    dd_hbm,
    out_ref,
    q_ref,
    nk_ref,
    nv_ref,
    cum_ref,
    flogit_ref,
    fbias_ref,
    len_ref,
    resid_ref,
    gain_ref,
    mix_ref,
    routes_ref,
    rw_ref,
    kc,
    vc,
    q_buf,
    nk_buf,
    nv_buf,
    lf_buf,
    len_buf,
    add_buf,
    score_buf,
    mix_buf,
    att_buf,
    ow,
    wgu,
    wd,
    dgu,
    pp_send,
    pp_recv,
    state_buf,
    norm_buf,
    gat,
    pf,
    psend,
    precv,
    aff,
    asend,
    arecv,
    hid,
    outs,
    cs_send,
    cs_recv,
    rs_send,
    rs_recv,
    small_sem,
    load_sem,
    cache_sem,
    pp_ssem,
    pp_rsem,
    ag_ssem,
    ag_rsem,
    p_ssem,
    p_rsem,
    h_ssem,
    h_rsem,
    c_ssem,
    c_rsem,
    rs_ssem,
    rs_rsem,
):
    ep_n, tp_n, sets, sent = dims
    ep = lax.axis_index("ep")
    tp = lax.axis_index("tp")
    f32, bf16 = jnp.float32, jnp.bfloat16
    tokens, width = out_ref.shape
    span = eg_hbm.shape[2]
    dspan = dg_hbm.shape[0]
    hidden = span + dspan
    chips = ep_n // 2
    chip = ep // 2
    core = lax.rem(ep, 2)
    partner = chip * 2 + 1 - core
    sizes = [2 * count * tokens for count, where, direct, whole in sets]
    firsts = [sum(sizes[:i]) for i in range(len(sets))]

    kv_local = kc.shape[1]
    heads = q_buf.shape[1]
    slots = kc.shape[2]
    grouping = heads // kv_local
    step = tokens // CACHE_CHUNKS
    cache = []
    for side, (src, dst) in enumerate(((kc_hbm, kc), (vc_hbm, vc))):
        for n in range(CACHE_CHUNKS):
            some = pl.ds(n * step, step)
            cache.append(
                pltpu.make_async_copy(src.at[some], dst.at[some], cache_sem.at[side, n])
            )
    smalls = [
        pltpu.make_async_copy(src, dst, small_sem.at[i % 7])
        for i, (src, dst) in enumerate(
            [
                (q_hbm, q_ref),
                (nk_hbm, nk_ref),
                (nv_hbm, nv_ref),
                (flogit_hbm, flogit_ref),
                (fbias_hbm, fbias_ref),
                (len_hbm, len_ref),
                (cum_hbm, cum_ref),
                (resid_hbm, resid_ref),
                (gain_hbm, gain_ref),
                (mix_hbm, mix_ref),
                (routes_hbm, routes_ref),
                (rw_hbm, rw_ref),
            ]
        )
    ]
    smalls[0].start()
    cache[0].start()
    for load in smalls[1:7]:
        load.start()
    for load in cache[1:]:
        load.start()
    loads = [
        pltpu.make_async_copy(src, dst, sem)
        for src, dst, sem in [
            (ow_hbm, ow, load_sem.at[0]),
            (dg_hbm, dgu.at[0:dspan], cache_sem.at[0, 0]),
            (du_hbm, dgu.at[dspan : 2 * dspan], cache_sem.at[0, 1]),
            (eg_hbm.at[0], wgu.at[:, 0:span], cache_sem.at[0, 2]),
            (eu_hbm.at[0], wgu.at[:, span : 2 * span], cache_sem.at[0, 3]),
            (ed_hbm.at[0], wd.at[0:span], cache_sem.at[1, 0]),
            (dd_hbm, wd.at[span:hidden], cache_sem.at[1, 1]),
        ]
    ]
    loads[0].start()

    barrier = pltpu.get_barrier_semaphore()
    for k in range(1, ep_n):
        pl.semaphore_signal(
            barrier, inc=1, device_id=(lax.rem(ep + k, ep_n), tp), device_id_type=MESH
        )
    for k in range(1, tp_n):
        pl.semaphore_signal(
            barrier, inc=1, device_id=(ep, lax.rem(tp + k, tp_n)), device_id_type=MESH
        )

    eye = lax.broadcasted_iota(jnp.int32, (tokens, tokens), 0) == lax.broadcasted_iota(
        jnp.int32, (tokens, tokens), 1
    )

    def column(row):
        return jnp.sum(jnp.where(eye, row, 0.0), axis=1, keepdims=True)

    q_buf[...] = jnp.zeros_like(q_buf)
    for load in smalls[0:6]:
        load.wait()
    for h in range(heads):
        g = h // grouping
        one = slice(g * HEAD, (g + 1) * HEAD)
        q_buf[:, h, one] = q_ref[:, h * HEAD : (h + 1) * HEAD].astype(f32)
        nk_buf[:, h, :] = nk_ref[...].astype(f32)
        nv_buf[:, h, :] = nv_ref[:, one].astype(f32)
        x = column(flogit_ref[h : h + 1, :]) + fbias_ref[h]
        lf_buf[:, h, :] = jnp.broadcast_to(
            jnp.minimum(x, 0.0) - jnp.log1p(jnp.exp(-jnp.abs(x))), (tokens, HEAD)
        )
    for load in smalls[7:]:
        load.start()
    head_row = lax.broadcasted_iota(jnp.int32, (heads, HEAD), 0)
    for n in range(tokens):
        len_buf[n] = jnp.full((heads, HEAD), len_ref[n], jnp.int32)

    def beside(ref, n):
        return jnp.concatenate([ref[n, g] for g in range(kv_local)], axis=1)

    scale = 1.0 / math.sqrt(HEAD)
    own = jnp.sum(q_buf[...] * nk_buf[...], axis=2, keepdims=True) * scale
    smalls[6].wait()
    cum = cum_ref[...]
    length = len_buf[:, :, 0:1]
    position = lax.broadcasted_iota(jnp.int32, (tokens, heads, slots), 2)
    latest = jnp.sum(jnp.where(position == length - 1, cum, 0.0), axis=2, keepdims=True)
    add_buf[...] = jnp.where(
        position < length, (latest + lf_buf[:, :, 0:1]) - cum, -jnp.inf
    )
    for n in range(tokens):
        if n % step == 0:
            cache[n // step].wait()
        score_buf[n] = lax.dot_general(
            q_buf[n].astype(bf16),
            beside(kc, n),
            (((1,), (1,)), ((), ())),
            preferred_element_type=f32,
        )
    for load in loads[1:5]:
        load.start()
    scores = score_buf[...] * scale + add_buf[...]
    highest = jnp.maximum(jnp.max(scores, axis=2, keepdims=True), own)
    past = jnp.exp(scores - highest)
    mine_own = jnp.exp(own - highest)
    totals = jnp.sum(past, axis=2, keepdims=True) + mine_own
    score_buf[...] = past / totals
    own_prob = (mine_own / totals).astype(bf16).astype(f32)
    for n in range(tokens):
        if n % step == 0:
            cache[CACHE_CHUNKS + n // step].wait()
        both = jnp.dot(score_buf[n].astype(bf16), beside(vc, n), preferred_element_type=f32)
        taken = both[:, 0:HEAD]
        for g in range(1, kv_local):
            taken = jnp.where(
                head_row >= g * grouping, both[:, g * HEAD : (g + 1) * HEAD], taken
            )
        mix_buf[n] = taken
    for load in loads[5:7]:
        load.start()
    mix_buf[...] = mix_buf[...] + own_prob * nv_buf[...]
    for h in range(heads):
        att_buf[:, h * HEAD : (h + 1) * HEAD] = mix_buf[:, h, :].astype(bf16)

    loads[0].wait()
    head_part = jnp.dot(att_buf[...], ow[...], preferred_element_type=f32)
    pp_send[...] = head_part.astype(bf16)
    pl.semaphore_wait(barrier, ep_n - 1 + tp_n - 1)

    def remote(src, dst, ssem, rsem, to):
        return pltpu.make_async_remote_copy(
            src_ref=src,
            dst_ref=dst,
            send_sem=ssem,
            recv_sem=rsem,
            device_id=to,
            device_id_type=MESH,
        )

    sends = []
    pp = []
    for k in range(1, tp_n):
        c = remote(
            pp_send,
            pp_recv.at[k - 1],
            pp_ssem.at[k - 1],
            pp_rsem.at[k - 1],
            (ep, lax.rem(tp + k, tp_n)),
        )
        c.start()
        pp.append(c)
        sends.append(c)
    for load in smalls[7:]:
        load.wait()
    loads[1].wait()
    loads[2].wait()
    wgu[:, 2 * span : 2 * hidden] = dgu[...].T
    for c in pp:
        c.wait_recv()
    projected = head_part
    for k in range(tp_n - 1):
        projected = projected + pp_recv[k].astype(f32)
    state_full = resid_ref[...].astype(f32) + projected.astype(bf16).astype(f32)
    inverse = lax.rsqrt(jnp.mean(state_full * state_full, axis=1, keepdims=True) + EPSILON)
    scaled_full = state_full * gain_ref[...]
    mix = mix_ref[...].astype(f32)
    mixed = jnp.zeros((tokens, HEAD), f32)
    for n in range(mix.shape[0]):
        mixed = mixed + scaled_full[:, n * HEAD : (n + 1) * HEAD] * mix[n : n + 1, :]
    gate = jax.nn.sigmoid(inverse * jnp.sum(mixed, axis=1, keepdims=True))
    state_buf[...] = state_full
    norm_buf[...] = scaled_full * inverse
    cols = pl.ds(pl.multiple_of(tp * width, 128), width)
    gat[core * chips + chip, :, 0:width] = norm_buf[:, cols].astype(bf16)
    lane = lax.broadcasted_iota(jnp.int32, (tokens, META), 1)
    named = [column(routes_ref[k : k + 1, :].astype(f32)) for k in range(TOP_K)]
    weighed = [column(rw_ref[k : k + 1, :]) for k in range(TOP_K)]
    meta = jnp.zeros((tokens, META), f32)
    for s in range(3):
        base = s * SEG
        value = jnp.where(lane == base, gate, 0.0)
        for k in range(TOP_K):
            value = value + jnp.where(
                (lane - base - 1).astype(f32) == named[k], weighed[k], 0.0
            )
        value = jnp.where((lane >= base) & (lane < base + SEG), value, 0.0)
        for cut in range(s):
            value = value - value.astype(bf16).astype(f32)
        meta = meta + value
    gat[core * chips + chip, :, width : width + META] = meta.astype(bf16)

    def put(src, dst, ssem, rsem, to):
        c = remote(src, dst, ssem, rsem, to)
        c.start()
        return c

    block = gat.at[core * chips + chip]
    gathers = [put(block, block, ag_ssem.at[0], ag_rsem.at[core, chip], (partner, tp))]

    def others(i):
        count, where, direct, whole = sets[i]
        first = where(chip)
        for b in range(count):
            if whole and b == 0:
                continue
            yield first + lax.rem(chip + b, count) if count > 1 else first

    def give(one, side, there, to):
        gathers.append(put(one, one, ag_ssem.at[0], ag_rsem.at[side, there], (to, tp)))

    for i in range(min(2, len(sets))):
        for there in others(i):
            give(block, core, chip, there * 2 + core)
            if sets[i][2]:
                give(block, core, chip, there * 2 + 1 - core)
    if sent is not None:
        deep = chips // PLANES
        for k in range(PLANES - 1):
            for b in range(deep):
                there = sent(k, chip) + lax.rem(chip + b, deep)
                give(block, core, chip, there * 2 + core)

    def arrive(side, there):
        came = gat.at[side * chips + there]
        remote(came, came, ag_ssem.at[0], ag_rsem.at[side, there], (partner, tp)).wait_recv()

    def forward(i):
        for there in others(i):
            arrive(core, there)
            came = gat.at[core * chips + there]
            if not sets[i][2]:
                give(came, core, there, partner)

    pcopies = {}
    hcopies = {}
    early = loads[3:5]
    late = loads[5:7]

    def piece(i, k):
        count, where, direct, whole = sets[i]
        share = 2 * count // tp_n
        at = k * share
        return gat.at[pl.ds(at // count * chips + where(chip) + lax.rem(at, count), share)]

    def everything(i):
        count, where, direct, whole = sets[i]
        return [gat.at[pl.ds(side * chips + where(chip), count)] for side in range(2)]

    def stage_in(i):
        count, where, direct, whole = sets[i]
        if direct:
            forward(i)
        if whole:
            arrive(1 - core, chip)
        for there in others(i):
            arrive(1 - core, there)
        while early:
            early.pop().wait()
        pcopies[i] = []
        if whole:
            pieces = everything(i)
        else:
            pieces = [piece(i, lax.rem(tp + k, tp_n)) for k in range(tp_n)]
        x = jnp.concatenate(
            [one[:, :, 0:width].reshape(sizes[i] // len(pieces), width) for one in pieces], axis=0
        )
        value = jnp.dot(x, wgu[...], preferred_element_type=f32)
        if whole:
            aff[...] = value
            asend[...] = value.astype(bf16)
        else:
            part = sizes[i] // tp_n
            at = pl.ds(firsts[i] // tp_n, part)
            pf[at] = value[0:part]
        for k in range(1, tp_n):
            if whole:
                src, dst = asend, arecv.at[k - 1]
            else:
                psend[k - 1, at] = value[k * part : (k + 1) * part].astype(bf16)
                src, dst = psend.at[k - 1, at], precv.at[k - 1, at]
            pcopies[i].append(
                put(
                    src,
                    dst,
                    p_ssem.at[int(whole), k - 1],
                    p_rsem.at[i, k - 1],
                    (ep, lax.rem(tp + k, tp_n)),
                )
            )

    expert = ep // EXP_SPAN

    def stage_mid(i):
        for c in pcopies[i]:
            c.wait_recv()
        whole = sets[i][3]
        hcopies[i] = []
        if whole:
            part, pieces = sizes[i], everything(i)
            own, other, at = aff, arecv, pl.ds(0, part)
        else:
            part, pieces = sizes[i] // tp_n, [piece(i, tp)]
            own, other, at = pf, precv, pl.ds(firsts[i] // tp_n, part)

        def total(low, size):
            value = own[at, low : low + size]
            for k in range(tp_n - 1):
                value = value + other[k, at, low : low + size].astype(f32)
            return value

        lanes = lax.broadcasted_iota(jnp.int32, (part, META), 1)
        info = jnp.concatenate(
            [
                one[:, :, width : width + META].reshape(part // len(pieces), META)
                for one in pieces
            ],
            axis=0,
        ).astype(f32)

        def picked(lane):
            spot = lanes - lane
            return jnp.sum(
                jnp.where((spot == 0) | (spot == SEG) | (spot == 2 * SEG), info, 0.0),
                axis=1,
                keepdims=True,
            )

        routed = picked(expert + 1) * jax.nn.silu(total(0, span)) * total(span, span)
        dense = picked(0) * jax.nn.silu(total(2 * span, dspan)) * total(2 * span + dspan, dspan)
        if whole:
            mine = pl.ds(firsts[i], part)
        else:
            mine = pl.ds(pl.multiple_of(firsts[i] + tp * part, 16), part)
        hid[mine, 0:span] = routed.astype(bf16)
        hid[mine, span:hidden] = dense.astype(bf16)
        if whole:
            return
        for k in range(1, tp_n):
            to = lax.rem(tp + k, tp_n)
            put(hid.at[mine], hid.at[mine], h_ssem.at[k - 1], h_rsem.at[i, k - 1], (ep, to))
            source = lax.rem(tp + tp_n - k, tp_n)
            theirs = pl.ds(pl.multiple_of(firsts[i] + source * part, 16), part)
            hcopies[i].append(
                remote(
                    hid.at[theirs],
                    hid.at[theirs],
                    h_ssem.at[k - 1],
                    h_rsem.at[i, k - 1],
                    (ep, to),
                )
            )

    ccopies = {}

    def stage_out(i):
        for c in hcopies[i]:
            c.wait_recv()
        while late:
            late.pop().wait()
        value = jnp.dot(
            hid[firsts[i] : firsts[i] + sizes[i]], wd[...], preferred_element_type=f32
        )
        half = sizes[i] // 2
        at = pl.ds(firsts[i] // 2, half)
        outs[0, at] = value[0:half]
        outs[1, at] = value[half : 2 * half]
        cs_send[at] = outs[1 - core, at].astype(bf16)
        ccopies[i] = put(
            cs_send.at[at], cs_recv.at[at], c_ssem.at[0], c_rsem.at[i], (partner, tp)
        )

    def stage_red(i):
        count, where, direct, whole = sets[i]
        ccopies[i].wait_recv()
        at = pl.ds(firsts[i] // 2, sizes[i] // 2)
        value = outs[core, at] + cs_recv[at].astype(f32)
        first = firsts[i] // 2 // tokens
        rs_send[pl.ds(first, count)] = value.astype(bf16).reshape(count, tokens, width)
        for b in range(count):
            slot = lax.rem(chip + b, count)
            if whole and b == 0:
                rs_recv[chip] = rs_send[first + slot]
                continue
            put(
                rs_send.at[first + slot],
                rs_recv.at[chip],
                rs_ssem.at[0],
                rs_rsem.at[0],
                ((where(chip) + slot) * 2 + core, tp),
            )

    stages = {
        "in": stage_in,
        "fwd": forward,
        "mid": stage_mid,
        "out": stage_out,
        "red": stage_red,
    }
    steps = STEPS
    if len(sets) == 1:
        steps = (("fwd", 0), ("in", 0), ("mid", 0), ("out", 0), ("red", 0))
    for stage, i in steps:
        stages[stage](i)

    def same(ref, ssem, rsem):
        return remote(ref, ref, ssem, rsem, (partner, tp))

    theirs = same(rs_recv.at[0 : chips - 1], rs_ssem.at[0], rs_rsem.at[0])
    theirs.wait_recv()
    result = state_buf[:, cols] + jnp.sum(rs_recv[...].astype(f32), axis=0)
    out_ref[...] = result.astype(bf16)
    theirs.wait_send()
    for c in sends:
        c.wait_send()
    same(gat.at[0 : len(gathers)], ag_ssem.at[0], ag_rsem.at[0, 0]).wait_send()
    same(cs_send, c_ssem.at[0], c_rsem.at[0]).wait_send()
    rest = (sum(sizes) - sizes[0]) // tp_n
    for k in range(tp_n - 1):
        same(asend, p_ssem.at[1, k], p_rsem.at[0, k]).wait_send()
        if rest:
            same(psend.at[k, 0:rest], p_ssem.at[0, k], p_rsem.at[0, k]).wait_send()
            same(hid.at[0:rest], h_ssem.at[k], h_rsem.at[0, k]).wait_send()


def plan(chips):
    planes = PLANES
    if chips % (2 * planes):
        return ((chips, lambda chip: 0, False, True),), None
    deep = chips // planes
    half = deep // 2

    def pick(table, k, chip):
        return sum(jnp.where(chip // deep == p, table[p][k], 0) for p in range(planes))

    def other(k, at):
        return lambda chip: pick(ORDER, k, chip) * deep + at

    sets = [
        (half, lambda chip: chip // half * half, False, True),
        (half, lambda chip: (chip // half ^ 1) * half, True, False),
    ]
    for k in range(planes - 1):
        if k in SPLIT:
            sets.append((half, other(k, 0), False, False))
            sets.append((half, other(k, half), False, False))
        else:
            sets.append((deep, other(k, 0), False, False))
    return tuple(sets), lambda k, chip: pick(SENDS, k, chip) * deep


def layer_call(
    q, nk, nv, cum, flogit, fbias, lengths, resid, gain, mix, routes, route_weight, kc, vc, ow, eg,
    eu, ed, dg, du, dd,
):
    ep_n, tp_n = lax.axis_size("ep"), lax.axis_size("tp")
    chips = ep_n // 2
    sets, sent = plan(chips)
    tokens, full = resid.shape
    width = full // tp_n
    rows = ep_n * tokens
    whole = 2 * sets[0][0] * tokens
    count = len(sets)
    span, dspan = eg.shape[2], dg.shape[0]
    hidden = span + dspan
    assert ep_n // EXP_SPAN + 1 <= SEG
    f32, bf16 = jnp.float32, jnp.bfloat16
    heads = cum.shape[1]
    vmem = pl.BlockSpec(memory_space=pltpu.VMEM)
    hbm = pl.BlockSpec(memory_space=pl.ANY)
    dma = pltpu.SemaphoreType.DMA
    peers = max(tp_n - 1, 1)
    return pl.pallas_call(
        functools.partial(layer_kernel, (ep_n, tp_n, sets, sent)),
        out_shape=pltpu.VMEM((tokens, width), bf16),
        in_specs=[hbm] * 21,
        out_specs=vmem,
        scratch_shapes=[
            pltpu.VMEM(q.shape, bf16),
            pltpu.VMEM(nk.shape, bf16),
            pltpu.VMEM(nv.shape, bf16),
            pltpu.VMEM(cum.shape, f32),
            pltpu.VMEM(flogit.shape, f32),
            pltpu.SMEM(fbias.shape, f32),
            pltpu.SMEM(lengths.shape, jnp.int32),
            pltpu.VMEM(resid.shape, bf16),
            pltpu.VMEM(gain.shape, f32),
            pltpu.VMEM(mix.shape, bf16),
            pltpu.VMEM(routes.shape, jnp.int32),
            pltpu.VMEM(route_weight.shape, f32),
            pltpu.VMEM(kc.shape, bf16),
            pltpu.VMEM(vc.shape, bf16),
            pltpu.VMEM((tokens, heads, nk.shape[1]), f32),
            pltpu.VMEM((tokens, heads, nk.shape[1]), f32),
            pltpu.VMEM((tokens, heads, HEAD), f32),
            pltpu.VMEM((tokens, heads, HEAD), f32),
            pltpu.VMEM((tokens, heads, HEAD), jnp.int32),
            pltpu.VMEM(cum.shape, f32),
            pltpu.VMEM(cum.shape, f32),
            pltpu.VMEM((tokens, heads, HEAD), f32),
            pltpu.VMEM((tokens, heads * HEAD), bf16),
            pltpu.VMEM(ow.shape, bf16),
            pltpu.VMEM((width, 2 * hidden), bf16),
            pltpu.VMEM((hidden, width), bf16),
            pltpu.VMEM((2 * dspan, width), bf16),
            pltpu.VMEM((tokens, full), bf16),
            pltpu.VMEM((peers, tokens, full), bf16),
            pltpu.VMEM((tokens, full), f32),
            pltpu.VMEM((tokens, full), f32),
            pltpu.VMEM((2 * chips, tokens, width + META), bf16),
            pltpu.VMEM((rows // tp_n, 2 * hidden), f32),
            pltpu.VMEM((peers, rows // tp_n, 2 * hidden), bf16),
            pltpu.VMEM((peers, rows // tp_n, 2 * hidden), bf16),
            pltpu.VMEM((whole, 2 * hidden), f32),
            pltpu.VMEM((whole, 2 * hidden), bf16),
            pltpu.VMEM((peers, whole, 2 * hidden), bf16),
            pltpu.VMEM((rows, hidden), bf16),
            pltpu.VMEM((2, rows // 2, width), f32),
            pltpu.VMEM((rows // 2, width), bf16),
            pltpu.VMEM((rows // 2, width), bf16),
            pltpu.VMEM((chips, tokens, width), bf16),
            pltpu.VMEM((chips, tokens, width), bf16),
            dma((7,)),
            dma((1,)),
            dma((2, CACHE_CHUNKS)),
            dma((peers,)),
            dma((peers,)),
            dma((1,)),
            dma((2, chips)),
            dma((2, peers)),
            dma((count, peers)),
            dma((peers,)),
            dma((count, peers)),
            dma((1,)),
            dma((count,)),
            dma((1,)),
            dma((1,)),
        ],
        compiler_params=pltpu.CompilerParams(
            collective_id=0, has_side_effects=True, vmem_limit_bytes=VMEM_LIMIT
        ),
        name="layer",
    )(
        q, nk, nv, cum, flogit, fbias, lengths, resid, gain, mix, routes, route_weight, kc, vc, ow,
        eg, eu, ed, dg, du, dd,
    )


def body(
    resid,
    queries,
    new_keys,
    new_values,
    key_cache,
    value_cache,
    cum_gate,
    forget_logit,
    forget_bias,
    lengths,
    out_weight,
    norm_gain,
    mix_vector,
    routes,
    route_weight,
    expert_gate,
    expert_up,
    expert_down,
    dense_gate,
    dense_up,
    dense_down,
):
    result = layer_call(
        queries,
        new_keys,
        new_values,
        cum_gate,
        forget_logit.T,
        forget_bias,
        lengths,
        resid,
        norm_gain.reshape(1, -1),
        mix_vector.reshape(-1, HEAD),
        routes.T,
        route_weight.T,
        key_cache,
        value_cache,
        out_weight,
        expert_gate,
        expert_up,
        expert_down,
        dense_gate.T,
        dense_up.T,
        dense_down,
    )
    return result


def solution(mesh):
    placed = (
        P("ep", None),
        P("ep", "tp"),
        P("ep", "tp"),
        P("ep", "tp"),
        P("ep", "tp", None, None),
        P("ep", "tp", None, None),
        P("ep", "tp", None),
        P("ep", "tp"),
        P("tp"),
        P("ep"),
        P("tp", None),
        P(),
        P(),
        P("ep", None),
        P("ep", None),
        P("ep", "tp", None),
        P("ep", "tp", None),
        P("ep", None, "tp"),
        P("tp", "ep"),
        P("tp", "ep"),
        P("ep", "tp"),
    )
    return jax.shard_map(body, mesh=mesh, in_specs=placed, out_specs=P("ep", "tp"), check_vma=False)
```

```python
import functools
import math

import jax
import jax.numpy as jnp
from jax import lax
from jax.experimental import pallas as pl
from jax.experimental.pallas import tpu as pltpu
from jax.sharding import PartitionSpec as P

HEAD = 128
TOP_K = 2
EXP_SPAN = 4


EPSILON = 1e-06
MESH = pl.DeviceIdType.MESH
META = 128
SEG = 42
PLANES = 4
ORDER = ((1, 2, 3), (0, 3, 2), (0, 3, 1), (0, 2, 1))
SENDS = ((2, 3, 1), (0, 2, 3), (1, 3, 0), (1, 2, 0))
SPLIT = (2,)
STEPS = (
    ("fwd", 0),
    ("in", 0),
    ("in", 1),
    ("fwd", 2),
    ("in", 2),
    ("fwd", 3),
    ("mid", 1),
    ("in", 3),
    ("fwd", 4),
    ("in", 4),
    ("fwd", 5),
    ("mid", 2),
    ("in", 5),
    ("mid", 0),
    ("out", 1),
    ("red", 1),
    ("mid", 3),
    ("out", 0),
    ("red", 0),
    ("mid", 4),
    ("out", 2),
    ("mid", 5),
    ("red", 2),
    ("out", 3),
    ("red", 3),
    ("out", 4),
    ("red", 4),
    ("out", 5),
    ("red", 5),
)
CACHE_CHUNKS = 4
VMEM_LIMIT = 60 * 1024 * 1024


def layer_kernel(
    dims,
    q_hbm,
    nk_hbm,
    nv_hbm,
    cum_hbm,
    flogit_hbm,
    fbias_hbm,
    len_hbm,
    resid_hbm,
    gain_hbm,
    mix_hbm,
    routes_hbm,
    rw_hbm,
    kc_hbm,
    vc_hbm,
    ow_hbm,
    eg_hbm,
    eu_hbm,
    ed_hbm,
    dg_hbm,
    du_hbm,
    dd_hbm,
    out_ref,
    q_ref,
    nk_ref,
    nv_ref,
    cum_ref,
    flogit_ref,
    fbias_ref,
    len_ref,
    resid_ref,
    gain_ref,
    mix_ref,
    routes_ref,
    rw_ref,
    kc,
    vc,
    q_buf,
    nk_buf,
    nv_buf,
    lf_buf,
    len_buf,
    add_buf,
    score_buf,
    mix_buf,
    att_buf,
    ow,
    wgu,
    wd,
    dgu,
    pp_send,
    pp_recv,
    state_buf,
    norm_buf,
    gat,
    pf,
    psend,
    precv,
    aff,
    asend,
    arecv,
    hid,
    outs,
    cs_send,
    cs_recv,
    rs_send,
    rs_recv,
    small_sem,
    load_sem,
    cache_sem,
    pp_ssem,
    pp_rsem,
    ag_ssem,
    ag_rsem,
    p_ssem,
    p_rsem,
    h_ssem,
    h_rsem,
    c_ssem,
    c_rsem,
    rs_ssem,
    rs_rsem,
):
    ep_n, tp_n, sets, sent = dims
    ep = lax.axis_index("ep")
    tp = lax.axis_index("tp")
    f32, bf16 = jnp.float32, jnp.bfloat16
    tokens, width = out_ref.shape
    span = eg_hbm.shape[2]
    dspan = dg_hbm.shape[0]
    hidden = span + dspan
    chips = ep_n // 2
    chip = ep // 2
    core = lax.rem(ep, 2)
    partner = chip * 2 + 1 - core
    sizes = [2 * count * tokens for count, where, direct, whole in sets]
    firsts = [sum(sizes[:i]) for i in range(len(sets))]

    kv_local = kc.shape[1]
    heads = q_buf.shape[1]
    slots = kc.shape[2]
    grouping = heads // kv_local
    step = tokens // CACHE_CHUNKS
    cache = []
    for side, (src, dst) in enumerate(((kc_hbm, kc), (vc_hbm, vc))):
        for n in range(CACHE_CHUNKS):
            some = pl.ds(n * step, step)
            cache.append(
                pltpu.make_async_copy(src.at[some], dst.at[some], cache_sem.at[side, n])
            )
    smalls = [
        pltpu.make_async_copy(src, dst, small_sem.at[i])
        for i, (src, dst) in enumerate(
            [
                (q_hbm, q_ref),
                (nk_hbm, nk_ref),
                (nv_hbm, nv_ref),
                (flogit_hbm, flogit_ref),
                (fbias_hbm, fbias_ref),
                (len_hbm, len_ref),
                (cum_hbm, cum_ref),
                (resid_hbm, resid_ref),
                (gain_hbm, gain_ref),
                (mix_hbm, mix_ref),
                (routes_hbm, routes_ref),
                (rw_hbm, rw_ref),
            ]
        )
    ]
    smalls[0].start()
    cache[0].start()
    for load in smalls[1:7]:
        load.start()
    for load in cache[1:]:
        load.start()
    loads = [
        pltpu.make_async_copy(src, dst, sem)
        for src, dst, sem in [
            (ow_hbm, ow, load_sem.at[0]),
            (dg_hbm, dgu.at[0:dspan], cache_sem.at[0, 0]),
            (du_hbm, dgu.at[dspan : 2 * dspan], cache_sem.at[0, 1]),
            (eg_hbm.at[0], wgu.at[:, 0:span], cache_sem.at[0, 2]),
            (eu_hbm.at[0], wgu.at[:, span : 2 * span], cache_sem.at[0, 3]),
            (ed_hbm.at[0], wd.at[0:span], cache_sem.at[1, 0]),
            (dd_hbm, wd.at[span:hidden], cache_sem.at[1, 1]),
        ]
    ]
    loads[0].start()
    for load in smalls[7:]:
        load.start()

    barrier = pltpu.get_barrier_semaphore()
    for k in range(1, ep_n):
        pl.semaphore_signal(
            barrier, inc=1, device_id=(lax.rem(ep + k, ep_n), tp), device_id_type=MESH
        )
    for k in range(1, tp_n):
        pl.semaphore_signal(
            barrier, inc=1, device_id=(ep, lax.rem(tp + k, tp_n)), device_id_type=MESH
        )

    eye = lax.broadcasted_iota(jnp.int32, (tokens, tokens), 0) == lax.broadcasted_iota(
        jnp.int32, (tokens, tokens), 1
    )

    def column(row):
        return jnp.sum(jnp.where(eye, row, 0.0), axis=1, keepdims=True)

    q_buf[...] = jnp.zeros_like(q_buf)
    for load in smalls[0:6]:
        load.wait()
    for h in range(heads):
        g = h // grouping
        one = slice(g * HEAD, (g + 1) * HEAD)
        q_buf[:, h, one] = q_ref[:, h * HEAD : (h + 1) * HEAD].astype(f32)
        nk_buf[:, h, :] = nk_ref[...].astype(f32)
        nv_buf[:, h, :] = nv_ref[:, one].astype(f32)
        x = column(flogit_ref[h : h + 1, :]) + fbias_ref[h]
        lf_buf[:, h, :] = jnp.broadcast_to(
            jnp.minimum(x, 0.0) - jnp.log1p(jnp.exp(-jnp.abs(x))), (tokens, HEAD)
        )
    head_row = lax.broadcasted_iota(jnp.int32, (heads, HEAD), 0)
    for n in range(tokens):
        len_buf[n] = jnp.full((heads, HEAD), len_ref[n], jnp.int32)

    def beside(ref, n):
        return jnp.concatenate([ref[n, g] for g in range(kv_local)], axis=1)

    scale = 1.0 / math.sqrt(HEAD)
    own = jnp.sum(q_buf[...] * nk_buf[...], axis=2, keepdims=True) * scale
    smalls[6].wait()
    cum = cum_ref[...]
    length = len_buf[:, :, 0:1]
    position = lax.broadcasted_iota(jnp.int32, (tokens, heads, slots), 2)
    latest = jnp.sum(jnp.where(position == length - 1, cum, 0.0), axis=2, keepdims=True)
    add_buf[...] = jnp.where(
        position < length, (latest + lf_buf[:, :, 0:1]) - cum, -jnp.inf
    )
    for n in range(tokens):
        if n % step == 0:
            cache[n // step].wait()
        score_buf[n] = lax.dot_general(
            q_buf[n].astype(bf16),
            beside(kc, n),
            (((1,), (1,)), ((), ())),
            preferred_element_type=f32,
        )
    for load in loads[1:5]:
        load.start()
    scores = score_buf[...] * scale + add_buf[...]
    highest = jnp.maximum(jnp.max(scores, axis=2, keepdims=True), own)
    past = jnp.exp(scores - highest)
    mine_own = jnp.exp(own - highest)
    totals = jnp.sum(past, axis=2, keepdims=True) + mine_own
    score_buf[...] = past / totals
    own_prob = (mine_own / totals).astype(bf16).astype(f32)
    for n in range(tokens):
        if n % step == 0:
            cache[CACHE_CHUNKS + n // step].wait()
        both = jnp.dot(score_buf[n].astype(bf16), beside(vc, n), preferred_element_type=f32)
        taken = both[:, 0:HEAD]
        for g in range(1, kv_local):
            taken = jnp.where(
                head_row >= g * grouping, both[:, g * HEAD : (g + 1) * HEAD], taken
            )
        mix_buf[n] = taken
    mix_buf[...] = mix_buf[...] + own_prob * nv_buf[...]
    for h in range(heads):
        att_buf[:, h * HEAD : (h + 1) * HEAD] = mix_buf[:, h, :].astype(bf16)

    loads[0].wait()
    head_part = jnp.dot(att_buf[...], ow[...], preferred_element_type=f32)
    pp_send[...] = head_part.astype(bf16)
    pl.semaphore_wait(barrier, ep_n - 1 + tp_n - 1)

    def remote(src, dst, ssem, rsem, to):
        return pltpu.make_async_remote_copy(
            src_ref=src,
            dst_ref=dst,
            send_sem=ssem,
            recv_sem=rsem,
            device_id=to,
            device_id_type=MESH,
        )

    sends = []
    pp = []
    for k in range(1, tp_n):
        c = remote(
            pp_send,
            pp_recv.at[k - 1],
            pp_ssem.at[k - 1],
            pp_rsem.at[k - 1],
            (ep, lax.rem(tp + k, tp_n)),
        )
        c.start()
        pp.append(c)
        sends.append(c)
    for load in loads[5:7]:
        load.start()
    for load in smalls[7:]:
        load.wait()
    loads[1].wait()
    loads[2].wait()
    wgu[:, 2 * span : 2 * hidden] = dgu[...].T
    for c in pp:
        c.wait_recv()
    projected = head_part
    for k in range(tp_n - 1):
        projected = projected + pp_recv[k].astype(f32)
    state_full = resid_ref[...].astype(f32) + projected.astype(bf16).astype(f32)
    inverse = lax.rsqrt(jnp.mean(state_full * state_full, axis=1, keepdims=True) + EPSILON)
    scaled_full = state_full * gain_ref[...]
    mix = mix_ref[...].astype(f32)
    mixed = jnp.zeros((tokens, HEAD), f32)
    for n in range(mix.shape[0]):
        mixed = mixed + scaled_full[:, n * HEAD : (n + 1) * HEAD] * mix[n : n + 1, :]
    gate = jax.nn.sigmoid(inverse * jnp.sum(mixed, axis=1, keepdims=True))
    state_buf[...] = state_full
    norm_buf[...] = scaled_full * inverse
    cols = pl.ds(pl.multiple_of(tp * width, 128), width)
    gat[core * chips + chip, :, 0:width] = norm_buf[:, cols].astype(bf16)
    lane = lax.broadcasted_iota(jnp.int32, (tokens, META), 1)
    named = [column(routes_ref[k : k + 1, :].astype(f32)) for k in range(TOP_K)]
    weighed = [column(rw_ref[k : k + 1, :]) for k in range(TOP_K)]
    meta = jnp.zeros((tokens, META), f32)
    for s in range(3):
        base = s * SEG
        value = jnp.where(lane == base, gate, 0.0)
        for k in range(TOP_K):
            value = value + jnp.where(
                (lane - base - 1).astype(f32) == named[k], weighed[k], 0.0
            )
        value = jnp.where((lane >= base) & (lane < base + SEG), value, 0.0)
        for cut in range(s):
            value = value - value.astype(bf16).astype(f32)
        meta = meta + value
    gat[core * chips + chip, :, width : width + META] = meta.astype(bf16)

    def put(src, dst, ssem, rsem, to):
        c = remote(src, dst, ssem, rsem, to)
        c.start()
        return c

    block = gat.at[core * chips + chip]
    gathers = [put(block, block, ag_ssem.at[0], ag_rsem.at[core, chip], (partner, tp))]

    def others(i):
        count, where, direct, whole = sets[i]
        first = where(chip)
        for b in range(count):
            if whole and b == 0:
                continue
            yield first + lax.rem(chip + b, count) if count > 1 else first

    def give(one, side, there, to):
        gathers.append(put(one, one, ag_ssem.at[0], ag_rsem.at[side, there], (to, tp)))

    for i in range(min(2, len(sets))):
        for there in others(i):
            give(block, core, chip, there * 2 + core)
            if sets[i][2]:
                give(block, core, chip, there * 2 + 1 - core)
    if sent is not None:
        deep = chips // PLANES
        for k in range(PLANES - 1):
            for b in range(deep):
                there = sent(k, chip) + lax.rem(chip + b, deep)
                give(block, core, chip, there * 2 + core)

    def arrive(side, there):
        came = gat.at[side * chips + there]
        remote(came, came, ag_ssem.at[0], ag_rsem.at[side, there], (partner, tp)).wait_recv()

    def forward(i):
        for there in others(i):
            arrive(core, there)
            came = gat.at[core * chips + there]
            if not sets[i][2]:
                give(came, core, there, partner)

    pcopies = {}
    hcopies = {}
    early = loads[3:5]
    late = loads[5:7]

    def piece(i, k):
        count, where, direct, whole = sets[i]
        share = 2 * count // tp_n
        at = k * share
        return gat.at[pl.ds(at // count * chips + where(chip) + lax.rem(at, count), share)]

    def everything(i):
        count, where, direct, whole = sets[i]
        return [gat.at[pl.ds(side * chips + where(chip), count)] for side in range(2)]

    def stage_in(i):
        count, where, direct, whole = sets[i]
        if direct:
            forward(i)
        if whole:
            arrive(1 - core, chip)
        for there in others(i):
            arrive(1 - core, there)
        while early:
            early.pop().wait()
        pcopies[i] = []
        if whole:
            pieces = everything(i)
        else:
            pieces = [piece(i, lax.rem(tp + k, tp_n)) for k in range(tp_n)]
        x = jnp.concatenate(
            [one[:, :, 0:width].reshape(sizes[i] // len(pieces), width) for one in pieces], axis=0
        )
        value = jnp.dot(x, wgu[...], preferred_element_type=f32)
        if whole:
            aff[...] = value
            asend[...] = value.astype(bf16)
        else:
            part = sizes[i] // tp_n
            at = pl.ds(firsts[i] // tp_n, part)
            pf[at] = value[0:part]
        for k in range(1, tp_n):
            if whole:
                src, dst = asend, arecv.at[k - 1]
            else:
                psend[k - 1, at] = value[k * part : (k + 1) * part].astype(bf16)
                src, dst = psend.at[k - 1, at], precv.at[k - 1, at]
            pcopies[i].append(
                put(
                    src,
                    dst,
                    p_ssem.at[int(whole), k - 1],
                    p_rsem.at[i, k - 1],
                    (ep, lax.rem(tp + k, tp_n)),
                )
            )

    expert = ep // EXP_SPAN

    def stage_mid(i):
        for c in pcopies[i]:
            c.wait_recv()
        whole = sets[i][3]
        hcopies[i] = []
        if whole:
            part, pieces = sizes[i], everything(i)
            own, other, at = aff, arecv, pl.ds(0, part)
        else:
            part, pieces = sizes[i] // tp_n, [piece(i, tp)]
            own, other, at = pf, precv, pl.ds(firsts[i] // tp_n, part)

        def total(low, size):
            value = own[at, low : low + size]
            for k in range(tp_n - 1):
                value = value + other[k, at, low : low + size].astype(f32)
            return value

        lanes = lax.broadcasted_iota(jnp.int32, (part, META), 1)
        info = jnp.concatenate(
            [
                one[:, :, width : width + META].reshape(part // len(pieces), META)
                for one in pieces
            ],
            axis=0,
        ).astype(f32)

        def picked(lane):
            spot = lanes - lane
            return jnp.sum(
                jnp.where((spot == 0) | (spot == SEG) | (spot == 2 * SEG), info, 0.0),
                axis=1,
                keepdims=True,
            )

        routed = picked(expert + 1) * jax.nn.silu(total(0, span)) * total(span, span)
        dense = picked(0) * jax.nn.silu(total(2 * span, dspan)) * total(2 * span + dspan, dspan)
        if whole:
            mine = pl.ds(firsts[i], part)
        else:
            mine = pl.ds(pl.multiple_of(firsts[i] + tp * part, 16), part)
        hid[mine, 0:span] = routed.astype(bf16)
        hid[mine, span:hidden] = dense.astype(bf16)
        if whole:
            return
        for k in range(1, tp_n):
            to = lax.rem(tp + k, tp_n)
            put(hid.at[mine], hid.at[mine], h_ssem.at[k - 1], h_rsem.at[i, k - 1], (ep, to))
            source = lax.rem(tp + tp_n - k, tp_n)
            theirs = pl.ds(pl.multiple_of(firsts[i] + source * part, 16), part)
            hcopies[i].append(
                remote(
                    hid.at[theirs],
                    hid.at[theirs],
                    h_ssem.at[k - 1],
                    h_rsem.at[i, k - 1],
                    (ep, to),
                )
            )

    ccopies = {}

    def stage_out(i):
        for c in hcopies[i]:
            c.wait_recv()
        while late:
            late.pop().wait()
        value = jnp.dot(
            hid[firsts[i] : firsts[i] + sizes[i]], wd[...], preferred_element_type=f32
        )
        half = sizes[i] // 2
        at = pl.ds(firsts[i] // 2, half)
        outs[0, at] = value[0:half]
        outs[1, at] = value[half : 2 * half]
        cs_send[at] = outs[1 - core, at].astype(bf16)
        ccopies[i] = put(
            cs_send.at[at], cs_recv.at[at], c_ssem.at[0], c_rsem.at[i], (partner, tp)
        )

    def stage_red(i):
        count, where, direct, whole = sets[i]
        ccopies[i].wait_recv()
        at = pl.ds(firsts[i] // 2, sizes[i] // 2)
        value = outs[core, at] + cs_recv[at].astype(f32)
        first = firsts[i] // 2 // tokens
        rs_send[pl.ds(first, count)] = value.astype(bf16).reshape(count, tokens, width)
        for b in range(count):
            slot = lax.rem(chip + b, count)
            if whole and b == 0:
                rs_recv[chip] = rs_send[first + slot]
                continue
            put(
                rs_send.at[first + slot],
                rs_recv.at[chip],
                rs_ssem.at[0],
                rs_rsem.at[0],
                ((where(chip) + slot) * 2 + core, tp),
            )

    stages = {
        "in": stage_in,
        "fwd": forward,
        "mid": stage_mid,
        "out": stage_out,
        "red": stage_red,
    }
    steps = STEPS
    if len(sets) == 1:
        steps = (("fwd", 0), ("in", 0), ("mid", 0), ("out", 0), ("red", 0))
    for stage, i in steps:
        stages[stage](i)

    def same(ref, ssem, rsem):
        return remote(ref, ref, ssem, rsem, (partner, tp))

    theirs = same(rs_recv.at[0 : chips - 1], rs_ssem.at[0], rs_rsem.at[0])
    theirs.wait_recv()
    result = state_buf[:, cols] + jnp.sum(rs_recv[...].astype(f32), axis=0)
    out_ref[...] = result.astype(bf16)
    theirs.wait_send()
    for c in sends:
        c.wait_send()
    same(gat.at[0 : len(gathers)], ag_ssem.at[0], ag_rsem.at[0, 0]).wait_send()
    same(cs_send, c_ssem.at[0], c_rsem.at[0]).wait_send()
    rest = (sum(sizes) - sizes[0]) // tp_n
    for k in range(tp_n - 1):
        same(asend, p_ssem.at[1, k], p_rsem.at[0, k]).wait_send()
        if rest:
            same(psend.at[k, 0:rest], p_ssem.at[0, k], p_rsem.at[0, k]).wait_send()
            same(hid.at[0:rest], h_ssem.at[k], h_rsem.at[0, k]).wait_send()


def plan(chips):
    planes = PLANES
    if chips % (2 * planes):
        return ((chips, lambda chip: 0, False, True),), None
    deep = chips // planes
    half = deep // 2

    def pick(table, k, chip):
        return sum(jnp.where(chip // deep == p, table[p][k], 0) for p in range(planes))

    def other(k, at):
        return lambda chip: pick(ORDER, k, chip) * deep + at

    sets = [
        (half, lambda chip: chip // half * half, False, True),
        (half, lambda chip: (chip // half ^ 1) * half, True, False),
    ]
    for k in range(planes - 1):
        if k in SPLIT:
            sets.append((half, other(k, 0), False, False))
            sets.append((half, other(k, half), False, False))
        else:
            sets.append((deep, other(k, 0), False, False))
    return tuple(sets), lambda k, chip: pick(SENDS, k, chip) * deep


def layer_call(
    q, nk, nv, cum, flogit, fbias, lengths, resid, gain, mix, routes, route_weight, kc, vc, ow, eg,
    eu, ed, dg, du, dd,
):
    ep_n, tp_n = lax.axis_size("ep"), lax.axis_size("tp")
    chips = ep_n // 2
    sets, sent = plan(chips)
    tokens, full = resid.shape
    width = full // tp_n
    rows = ep_n * tokens
    whole = 2 * sets[0][0] * tokens
    count = len(sets)
    span, dspan = eg.shape[2], dg.shape[0]
    hidden = span + dspan
    assert ep_n // EXP_SPAN + 1 <= SEG
    f32, bf16 = jnp.float32, jnp.bfloat16
    heads = cum.shape[1]
    vmem = pl.BlockSpec(memory_space=pltpu.VMEM)
    hbm = pl.BlockSpec(memory_space=pl.ANY)
    dma = pltpu.SemaphoreType.DMA
    peers = max(tp_n - 1, 1)
    return pl.pallas_call(
        functools.partial(layer_kernel, (ep_n, tp_n, sets, sent)),
        out_shape=pltpu.VMEM((tokens, width), bf16),
        in_specs=[hbm] * 21,
        out_specs=vmem,
        scratch_shapes=[
            pltpu.VMEM(q.shape, bf16),
            pltpu.VMEM(nk.shape, bf16),
            pltpu.VMEM(nv.shape, bf16),
            pltpu.VMEM(cum.shape, f32),
            pltpu.VMEM(flogit.shape, f32),
            pltpu.SMEM(fbias.shape, f32),
            pltpu.SMEM(lengths.shape, jnp.int32),
            pltpu.VMEM(resid.shape, bf16),
            pltpu.VMEM(gain.shape, f32),
            pltpu.VMEM(mix.shape, bf16),
            pltpu.VMEM(routes.shape, jnp.int32),
            pltpu.VMEM(route_weight.shape, f32),
            pltpu.VMEM(kc.shape, bf16),
            pltpu.VMEM(vc.shape, bf16),
            pltpu.VMEM((tokens, heads, nk.shape[1]), f32),
            pltpu.VMEM((tokens, heads, nk.shape[1]), f32),
            pltpu.VMEM((tokens, heads, HEAD), f32),
            pltpu.VMEM((tokens, heads, HEAD), f32),
            pltpu.VMEM((tokens, heads, HEAD), jnp.int32),
            pltpu.VMEM(cum.shape, f32),
            pltpu.VMEM(cum.shape, f32),
            pltpu.VMEM((tokens, heads, HEAD), f32),
            pltpu.VMEM((tokens, heads * HEAD), bf16),
            pltpu.VMEM(ow.shape, bf16),
            pltpu.VMEM((width, 2 * hidden), bf16),
            pltpu.VMEM((hidden, width), bf16),
            pltpu.VMEM((2 * dspan, width), bf16),
            pltpu.VMEM((tokens, full), bf16),
            pltpu.VMEM((peers, tokens, full), bf16),
            pltpu.VMEM((tokens, full), f32),
            pltpu.VMEM((tokens, full), f32),
            pltpu.VMEM((2 * chips, tokens, width + META), bf16),
            pltpu.VMEM((rows // tp_n, 2 * hidden), f32),
            pltpu.VMEM((peers, rows // tp_n, 2 * hidden), bf16),
            pltpu.VMEM((peers, rows // tp_n, 2 * hidden), bf16),
            pltpu.VMEM((whole, 2 * hidden), f32),
            pltpu.VMEM((whole, 2 * hidden), bf16),
            pltpu.VMEM((peers, whole, 2 * hidden), bf16),
            pltpu.VMEM((rows, hidden), bf16),
            pltpu.VMEM((2, rows // 2, width), f32),
            pltpu.VMEM((rows // 2, width), bf16),
            pltpu.VMEM((rows // 2, width), bf16),
            pltpu.VMEM((chips, tokens, width), bf16),
            pltpu.VMEM((chips, tokens, width), bf16),
            dma((12,)),
            dma((1,)),
            dma((2, CACHE_CHUNKS)),
            dma((peers,)),
            dma((peers,)),
            dma((1,)),
            dma((2, chips)),
            dma((2, peers)),
            dma((count, peers)),
            dma((peers,)),
            dma((count, peers)),
            dma((1,)),
            dma((count,)),
            dma((1,)),
            dma((1,)),
        ],
        compiler_params=pltpu.CompilerParams(
            collective_id=0, has_side_effects=True, vmem_limit_bytes=VMEM_LIMIT
        ),
        name="layer",
    )(
        q, nk, nv, cum, flogit, fbias, lengths, resid, gain, mix, routes, route_weight, kc, vc, ow,
        eg, eu, ed, dg, du, dd,
    )


def body(
    resid,
    queries,
    new_keys,
    new_values,
    key_cache,
    value_cache,
    cum_gate,
    forget_logit,
    forget_bias,
    lengths,
    out_weight,
    norm_gain,
    mix_vector,
    routes,
    route_weight,
    expert_gate,
    expert_up,
    expert_down,
    dense_gate,
    dense_up,
    dense_down,
):
    result = layer_call(
        queries,
        new_keys,
        new_values,
        cum_gate,
        forget_logit.T,
        forget_bias,
        lengths,
        resid,
        norm_gain.reshape(1, -1),
        mix_vector.reshape(-1, HEAD),
        routes.T,
        route_weight.T,
        key_cache,
        value_cache,
        out_weight,
        expert_gate,
        expert_up,
        expert_down,
        dense_gate.T,
        dense_up.T,
        dense_down,
    )
    return result


def solution(mesh):
    placed = (
        P("ep", None),
        P("ep", "tp"),
        P("ep", "tp"),
        P("ep", "tp"),
        P("ep", "tp", None, None),
        P("ep", "tp", None, None),
        P("ep", "tp", None),
        P("ep", "tp"),
        P("tp"),
        P("ep"),
        P("tp", None),
        P(),
        P(),
        P("ep", None),
        P("ep", None),
        P("ep", "tp", None),
        P("ep", "tp", None),
        P("ep", None, "tp"),
        P("tp", "ep"),
        P("tp", "ep"),
        P("ep", "tp"),
    )
    return jax.shard_map(body, mesh=mesh, in_specs=placed, out_specs=P("ep", "tp"), check_vma=False)
```
